128 devices in a mesh: sp: 16 (over z, y), dp: 8 (over x, core).
Axes of the slice: x: 4, y: 4, z: 4, core: 2. Of those that a mesh axis runs over, the one named last changes fastest.
Arguments:
- layer_input: bfloat16 [8, 2048, 2048], P('dp', 'sp'), may hold values from -0.0390625 to 0.0390625
- queries: bfloat16 [8, 2048, 2048], P('dp', 'sp'), may hold values from -6 to 6
- key_vectors: bfloat16 [8, 2048, 2048], P('dp', 'sp'), may hold values from -6 to 6
- values: bfloat16 [8, 2048, 4096], P('dp', 'sp'), may hold values from -6 to 6
- cotangent: bfloat16 [8, 2048, 4096], P('dp', 'sp'), may hold values from -0.3125 to 0.3125
- log_decay: float32 [8, 16, 2048], P('dp', 'sp'), may hold values from -3 to 0
- key_weight: bfloat16 [2048, 2048], P('dp'), may hold values from -0.125 to 0.125
Outputs:
- grad_query: bfloat16 [8, 2048, 2048], P('dp', 'sp')
- grad_value: bfloat16 [8, 2048, 4096], P('dp', 'sp')
- grad_input: bfloat16 [8, 2048, 2048], P('dp', 'sp')
- grad_key_weight: float32 [2048, 2048], P('dp')
The draws below stay inside these ranges and needn't reach their ends.
All inputs are finite; a program needn't handle non-finite values.
Results may differ from the reference program's by a relative error of at most 0.012.
Values may be sent and summed in bfloat16 or wider, within the bound.
No kernel may reach another device: no remote copies, remote signals or barrier semaphores. Data moves between devices by JAX's collectives and lax.ppermute only.
A program may use at most 128 MiB of HBM per device.

```python
import jax
import jax.numpy as jnp
from jax import lax

D = 2048
HEADS = 8
DK = 256
DV = 512
BLOCK = 128
TOK_DEV = 128
HEAD_DIRECTIONS = 16
SEQUENCE_LENGTH = 2048
SEQUENCE_COUNT = 8
HK = 2048
HV = 4096


def draw_log_decay(key, part):
    parallel_lanes = jax.random.split(jax.random.fold_in(key, 71), 6)
    fast_share = 0.5
    is_fast = jax.random.uniform(parallel_lanes[0], (SEQUENCE_COUNT, HEAD_DIRECTIONS, 1)) < fast_share
    fast_rate = jnp.exp(jax.random.uniform(parallel_lanes[1], (SEQUENCE_COUNT, HEAD_DIRECTIONS, 1), jnp.float32, jnp.log(2.0), jnp.log(6.0))) / BLOCK
    slow_rate = jnp.ones((SEQUENCE_COUNT, HEAD_DIRECTIONS, 1), jnp.float32) / SEQUENCE_LENGTH
    baseline_decay_rate = jnp.where(is_fast, fast_rate, slow_rate)
    block_multiplier = jnp.exp(jax.random.uniform(parallel_lanes[2], (SEQUENCE_COUNT, HEAD_DIRECTIONS, SEQUENCE_LENGTH // TOK_DEV), jnp.float32, jnp.log(0.5), jnp.log(2.0)))
    block_multiplier = jnp.repeat(block_multiplier, TOK_DEV, axis=2)
    decay_jitter = jax.random.uniform(parallel_lanes[3], (SEQUENCE_COUNT, HEAD_DIRECTIONS, SEQUENCE_LENGTH), jnp.float32, 0.5, 1.5)
    group_position = jax.random.randint(parallel_lanes[4], (SEQUENCE_COUNT, HEAD_DIRECTIONS, 2), 0, SEQUENCE_LENGTH)
    group_depth = jnp.log(jax.random.uniform(parallel_lanes[5], (SEQUENCE_COUNT, HEAD_DIRECTIONS, 2), jnp.float32, 0.5, 0.8))
    position_slots = jnp.arange(SEQUENCE_LENGTH)[None, None, None, :]
    token_groups = jnp.sum(jnp.where(position_slots == group_position[..., None], group_depth[..., None], 0.0), axis=2)
    return (-baseline_decay_rate * block_multiplier * decay_jitter + token_groups).astype(jnp.float32)


def with_spikes(drawn, own_key, source, target, blocks, factor):
    def block_of(axis_at):
        return (jnp.arange(drawn.shape[axis_at]) // (drawn.shape[axis_at] // blocks)).reshape((-1,) + (1,) * (drawn.ndim - 1 - axis_at))

    near = jax.random.permutation(own_key, blocks)[block_of(target)]
    other_side = (block_of(target) + blocks // 2) % blocks
    return jnp.where((block_of(source) == near) | (block_of(source) == other_side), factor * drawn, drawn)


def level_of(rng, shape, cuts, least, largest):
    loudness, own = 1.0, jax.random.fold_in(rng, 6)
    for dim, shards_of in cuts:
        draws = jnp.exp(jax.random.uniform(jax.random.fold_in(own, dim), (shards_of,), jnp.float32, least / len(cuts), largest / len(cuts)))
        loudness = loudness * jnp.repeat(draws, shape[dim] // shards_of).reshape([-1 if axis == dim else 1 for axis in range(len(shape))])
    return loudness


def scatter_about(rng, dims, scale, reach, cuts=(), held_as=jnp.bfloat16):
    gain = level_of(rng, dims, cuts, -0.22, 0.18) if cuts else 1.0
    drawn = jax.random.normal(rng, dims, jnp.float32) * scale * gain
    return jnp.minimum(jnp.maximum(drawn, -reach), reach).astype(held_as)


def heavy_noise(own_key, shape, width, most, shards, heavy, kind=jnp.bfloat16):
    values = width * jax.random.normal(own_key, shape, jnp.float32)
    if shards:
        values = values * level_of(own_key, shape, shards, -0.22, 0.18)
    return jnp.clip(with_spikes(values, jax.random.fold_in(own_key, 3), *heavy), -most, most).astype(kind)


def setup_inputs(seed: int = 0) -> dict:
    streams_of = jax.random.split(jax.random.key(seed), 8)
    layer_input = heavy_noise(streams_of[0], (SEQUENCE_COUNT, SEQUENCE_LENGTH, D), 0.005, 0.0390625, ((0, 8), (1, 16)), (1, 2, 16, 2.0))
    queries = scatter_about(streams_of[1], (SEQUENCE_COUNT, SEQUENCE_LENGTH, HK), 1.0, 6.0, ((0, 8), (1, 16)))
    key_vectors = scatter_about(streams_of[2], (SEQUENCE_COUNT, SEQUENCE_LENGTH, HK), 1.0, 6.0, ((0, 8), (1, 16)))
    values = scatter_about(streams_of[3], (SEQUENCE_COUNT, SEQUENCE_LENGTH, HV), 1.0, 6.0, ((0, 8), (1, 16)))
    cotangent = scatter_about(streams_of[4], (SEQUENCE_COUNT, SEQUENCE_LENGTH, HV), 0.05, 0.3125, ((0, 8), (1, 16)))
    log_decay = draw_log_decay(jax.random.fold_in(streams_of[7], 71), 0)
    key_weight = scatter_about(streams_of[6], (D, HK), D ** -0.5, 0.125, ((0, 8),))
    return {"layer_input": layer_input, "queries": queries, "key_vectors": key_vectors, "values": values, "cotangent": cotangent, "log_decay": log_decay, "key_weight": key_weight}


def unit_backward(query_rows, key_rows, value_rows, grad_rows, decay_rows, strict):
    length, key_width = query_rows.shape
    value_width = value_rows.shape[1]
    blocks = length // BLOCK
    scaling = key_width ** -0.5
    query_blk = query_rows.reshape(blocks, BLOCK, key_width)
    key_blk = key_rows.reshape(blocks, BLOCK, key_width)
    value_blk = value_rows.reshape(blocks, BLOCK, value_width)
    grad_blk = grad_rows.reshape(blocks, BLOCK, value_width)
    within = jnp.cumsum(decay_rows.reshape(blocks, BLOCK), axis=1)
    position_slots = jnp.arange(BLOCK)
    allowed = jnp.where(strict, position_slots[None, :] < position_slots[:, None], position_slots[None, :] <= position_slots[:, None])
    spread = jnp.where(allowed, within[:, :, None] - within[:, None, :], 0.0)
    weights = jnp.where(allowed, jnp.exp(spread), 0.0) * scaling
    raw_scores = jnp.einsum("nid,njd->nij", query_blk, key_blk, preferred_element_type=jnp.float32)
    scores = (raw_scores * weights).astype(jnp.bfloat16)
    raw_grads = jnp.einsum("niv,njv->nij", grad_blk, value_blk, preferred_element_type=jnp.float32)
    grad_scores = (raw_grads * weights).astype(jnp.bfloat16)
    value_inner = jnp.einsum("nij,niv->njv", scores, grad_blk, preferred_element_type=jnp.float32)
    query_inner = jnp.einsum("nij,njd->nid", grad_scores, key_blk, preferred_element_type=jnp.float32)
    key_inner = jnp.einsum("nij,nid->njd", grad_scores, query_blk, preferred_element_type=jnp.float32)
    ending = within[:, -1:]
    query_scale = jnp.exp(within) * scaling
    key_scale = jnp.exp(ending - within)
    carry_decay = jnp.exp(ending[:, 0])
    query_dec = (query_blk * query_scale[:, :, None]).astype(jnp.bfloat16)
    key_dec = (key_blk * key_scale[:, :, None]).astype(jnp.bfloat16)
    contract = (((0,), (0,)), ((), ()))

    def advance(memory, inputs):
        key_b, value_b, factor = inputs
        before = memory.astype(jnp.bfloat16)
        memory = factor * memory + lax.dot_general(key_b, value_b, contract, preferred_element_type=jnp.float32)
        return memory, before

    start_state = jnp.zeros((key_width, value_width), jnp.float32)
    _, states_before = lax.scan(advance, start_state, (key_dec, value_blk, carry_decay))

    def retreat(later, inputs):
        query_b, grad_b, factor = inputs
        after = later.astype(jnp.bfloat16)
        later = factor * later + lax.dot_general(query_b, grad_b, contract, preferred_element_type=jnp.float32)
        return later, after

    _, state_grads = lax.scan(retreat, start_state, (query_dec, grad_blk, carry_decay), reverse=True)
    query_carried = jnp.einsum("niv,ndv->nid", grad_blk, states_before, preferred_element_type=jnp.float32)
    key_carried = jnp.einsum("njv,ndv->njd", value_blk, state_grads, preferred_element_type=jnp.float32)
    value_carried = jnp.einsum("njd,ndv->njv", key_dec, state_grads, preferred_element_type=jnp.float32)
    grad_q = query_inner + query_carried * query_scale[:, :, None]
    grad_k = key_inner + key_carried * key_scale[:, :, None]
    grad_v = value_inner + value_carried
    return (grad_q.reshape(length, key_width), grad_k.reshape(length, key_width),
            grad_v.reshape(length, value_width))


def unit_grads(query_rows, key_rows, value_rows, grad_rows, decay_rows, backward):
    def orient(array):
        return jnp.where(backward, jnp.flip(array, 0), array)

    gradients = unit_backward(orient(query_rows), orient(key_rows), orient(value_rows),
                              orient(grad_rows), orient(decay_rows), backward)
    return tuple(orient(single).astype(jnp.bfloat16) for single in gradients)


def reference(layer_input, queries, key_vectors, values, cotangent, log_decay, key_weight):
    def one_sequence(inputs):
        rows_in, query_seq, key_seq, value_seq, grad_seq, decay_seq = inputs
        length = query_seq.shape[0]
        query_heads = query_seq.reshape(length, HEADS, DK)
        key_heads = key_seq.reshape(length, HEADS, DK)
        value_heads = value_seq.reshape(length, HEADS, DV)
        grad_heads = grad_seq.reshape(length, HEADS, DV)
        query_list, key_list, value_list = [], [], []
        for head_index in range(HEADS):
            halves = [unit_grads(query_heads[:, head_index], key_heads[:, head_index], value_heads[:, head_index],
                                 grad_heads[:, head_index], decay_seq[2 * head_index + direction], direction == 1)
                      for direction in range(2)]
            paired = [(halves[0][slot].astype(jnp.float32) + halves[1][slot].astype(jnp.float32)).astype(jnp.bfloat16)
                      for slot in range(3)]
            query_list.append(paired[0])
            key_list.append(paired[1])
            value_list.append(paired[2])
        grad_query = jnp.concatenate(query_list, axis=1)
        grad_key = jnp.concatenate(key_list, axis=1)
        grad_value = jnp.concatenate(value_list, axis=1)
        grad_input = jnp.dot(grad_key, key_weight.T, preferred_element_type=jnp.float32).astype(jnp.bfloat16)
        local_term = jnp.dot(rows_in.T, grad_key, preferred_element_type=jnp.float32)
        return grad_query, grad_value, grad_input, local_term

    outputs = lax.map(one_sequence, (layer_input, queries, key_vectors, values, cotangent, log_decay))
    return outputs[0], outputs[1], outputs[2], jnp.sum(outputs[3], axis=0)
```

```python
import jax
import jax.numpy as jnp
from jax import lax
from jax.experimental import pallas as pl
from jax.experimental.pallas import tpu as pltpu
from jax.sharding import Mesh
from jax.sharding import PartitionSpec as P

HEADS = 8
BLOCK = 128
TILE = 256
SP = ("half", "lane")
DP = ("dp_0", "dp_1")
F32 = jnp.float32
BF16 = jnp.bfloat16


def dot(a, b, dims, precision=None):
    return lax.dot_general(a, b, (dims, ((), ())), precision=precision, preferred_element_type=F32)


NN = ((1,), (0,))
NT = ((1,), (1,))
TN = ((0,), (0,))


def decay_kernel(lam_ref, half_ref, rows_ref, cols_ref):
    n = BLOCK
    row = lax.broadcasted_iota(jnp.int32, (n, n), 0)
    col = lax.broadcasted_iota(jnp.int32, (n, n), 1)
    lam = lam_ref[...]
    high = lax.Precision.HIGHEST
    upto = dot(lam, (row <= col).astype(F32), NN, high)
    before = dot(lam, (row < col).astype(F32), NN, high)
    since = dot(lam, (row >= col).astype(F32), NN, high)
    after = dot(lam, (row > col).astype(F32), NN, high)
    totals = [jnp.broadcast_to(upto[b : b + 1, n - 1 : n], (1, n)) for b in range(16)]
    loc0, suf1, rem0, pre1 = [], [], [], []
    for b in range(8):
        odd = b % 2 == 1
        loc0.append(upto[b : b + 1] + totals[b - 1] if odd else upto[b : b + 1])
        suf1.append(since[8 + b : 9 + b] if odd else since[8 + b : 9 + b] + totals[9 + b])
        rem0.append(after[b : b + 1] if odd else after[b : b + 1] + totals[b + 1])
        pre1.append(before[8 + b : 9 + b] + totals[7 + b] if odd else before[8 + b : 9 + b])
    tile0 = [totals[2 * t] + totals[2 * t + 1] for t in range(4)]
    tile1 = [totals[8 + 2 * t] + totals[9 + 2 * t] for t in range(4)]
    first = half_ref[...] == 0
    key_sum, query_sum = [], []
    for b in range(8):
        t = b // 2
        later0, later1 = sum(tile0[t + 1 :]), sum(tile1[t + 1 :])
        early0, early1 = sum(tile0[:t]), sum(tile1[:t])
        key_sum.append(jnp.where(first, rem0[b] + later0, pre1[b] + early1))
        query_sum.append(jnp.where(first, suf1[b] + later1, loc0[b] + early0))
    rows_ref[...] = jnp.concatenate(loc0 + suf1 + rem0 + pre1 + tile0 + tile1, axis=0)
    keys = jnp.exp(jnp.concatenate(key_sum, axis=0))
    queries = jnp.exp(jnp.concatenate(query_sum, axis=0)) * 0.0625
    stack = [jnp.concatenate(loc0 + suf1, axis=0), keys, queries, jnp.zeros((n - 32, n), F32)]
    cols_ref[...] = jnp.transpose(jnp.concatenate(stack, axis=0))


def tall(cols, base, block_pair=None):
    picks = range(8) if block_pair is None else (2 * block_pair, 2 * block_pair + 1)
    return jnp.concatenate([cols[:, base + b : base + b + 1] for b in picks], axis=0)


def wide(rows, base, t):
    return jnp.concatenate([rows[base + 2 * t : base + 2 * t + 1], rows[base + 2 * t + 1 : base + 2 * t + 2]], axis=1)


def boundary_kernel(units_ref, cols_ref, state_ref, keys_ref):
    cols = cols_ref[...]
    keys = (units_ref[:, 256:512].astype(F32) * tall(cols, 16)).astype(BF16)
    queries = (units_ref[:, 0:256].astype(F32) * tall(cols, 24)).astype(BF16)
    keys_ref[...] = keys
    state_ref[0] = dot(keys, units_ref[:, 512:1024], TN).astype(BF16)
    state_ref[1] = dot(queries, units_ref[:, 1024:1536], TN).astype(BF16)


def inside_kernel(units_ref, rows_ref, cols_ref, out_ref, s_ref, gs_ref):
    rows, cols = rows_ref[...], cols_ref[...]
    row = lax.broadcasted_iota(jnp.int32, (TILE, TILE), 0)
    col = lax.broadcasted_iota(jnp.int32, (TILE, TILE), 1)
    for i in range(4):
        at = pl.ds(i * TILE, TILE)
        query, grad = units_ref[at, 0:256], units_ref[at, 1024:1536]
        loc0, suf1 = tall(cols, 0, i), tall(cols, 8, i)
        for j in range(4):
            to = pl.ds(j * TILE, TILE)
            if i == j:
                spread = jnp.where(row >= col, loc0 - wide(rows, 0, i), suf1 - wide(rows, 8, i))
            elif i > j:
                along = wide(rows, 16, j)
                for t in range(j + 1, i):
                    along = along + jnp.concatenate([rows[32 + t : 33 + t]] * 2, axis=1)
                spread = loc0 + along
            else:
                along = wide(rows, 24, j)
                for t in range(i + 1, j):
                    along = along + jnp.concatenate([rows[36 + t : 37 + t]] * 2, axis=1)
                spread = suf1 + along
            weights = jnp.exp(spread) * 0.0625
            scores = dot(query, units_ref[to, 256:512], NT)
            grads = dot(grad, units_ref[to, 512:1024], NT)
            s_ref[at, to] = (scores * weights).astype(BF16)
            gs_ref[at, to] = (grads * weights).astype(BF16)
    out_ref[:, 0:256] = dot(gs_ref[...], units_ref[:, 0:256], TN)
    out_ref[:, 256:512] = dot(gs_ref[...], units_ref[:, 256:512], NN)
    out_ref[:, 512:1024] = dot(s_ref[...], units_ref[:, 1024:1536], TN)


def across_kernel(units_ref, cols_ref, keys_ref, state_ref, part_ref, out_ref):
    cols = cols_ref[...]
    memory, later = state_ref[0], state_ref[1]
    key_part = dot(units_ref[:, 512:1024], later, NT) * tall(cols, 16)
    out_ref[:, 0:256] = (part_ref[:, 0:256] + key_part).astype(BF16)
    query_part = dot(units_ref[:, 1024:1536], memory, NT) * tall(cols, 24)
    out_ref[:, 256:512] = (part_ref[:, 256:512] + query_part).astype(BF16)
    value_part = dot(keys_ref[...], later, NN)
    out_ref[:, 512:1024] = (part_ref[:, 512:1024] + value_part).astype(BF16)


def kernel(body, out_shape, flops, scratch=()):
    return pl.pallas_call(
        body,
        out_shape=out_shape,
        scratch_shapes=scratch,
        cost_estimate=pl.CostEstimate(flops=flops, bytes_accessed=4 << 20, transcendentals=0),
        compiler_params=pltpu.CompilerParams(vmem_limit_bytes=48 << 20),
    )


def shape(dims, dtype):
    return jax.ShapeDtypeStruct(dims, dtype)


def shards(layer_input, queries, key_vectors, values, cotangent, log_decay, key_weight):
    tokens = layer_input.shape[1]
    half = lax.axis_index("half")
    peers = lax.axis_size(SP)
    weight = lax.all_gather(key_weight, DP, tiled=True)

    decay = log_decay.reshape(2, 8, BLOCK)
    own = lax.axis_index("lane") % 2
    near = lax.dynamic_index_in_dim(decay, own, 0, keepdims=False)
    far = lax.dynamic_index_in_dim(decay, 1 - own, 0, keepdims=False)
    near = lax.ppermute(near, SP, [(u, u % 2 * 8 + u // 2) for u in range(peers)])
    far = lax.ppermute(far, SP, [(u, (1 - u % 2) * 8 + u // 2) for u in range(peers)])
    lam = jnp.where(half == 0, jnp.concatenate([near, far]), jnp.concatenate([far, near]))
    rows, cols = kernel(decay_kernel, (shape((40, 128), F32), shape((128, 128), F32)), 1 << 20)(
        lam, jnp.full((1, 128), half, jnp.int32)
    )

    def by_head(array):
        return jnp.moveaxis(array[0].reshape(tokens, HEADS, -1), 1, 0)

    sent = jnp.concatenate([by_head(a) for a in (queries, key_vectors, values, cotangent)], axis=2)
    units = lax.all_to_all(sent, "lane", 0, 0, tiled=True).reshape(8 * tokens, -1)
    gathered = lax.all_gather(layer_input[0], "lane", tiled=True)

    state, keys = kernel(
        boundary_kernel, (shape((2, 256, 512), BF16), shape((1024, 256), BF16)), 540 << 20
    )(units, cols)
    state = lax.ppermute(state, SP, [(u, (u + 8) % 16) for u in range(peers)])
    part = kernel(
        inside_kernel,
        shape((1024, 1024), F32),
        3760 << 20,
        (pltpu.VMEM((1024, 1024), BF16), pltpu.VMEM((1024, 1024), BF16)),
    )(units, rows, cols)
    grads = kernel(across_kernel, shape((1024, 1024), BF16), 800 << 20)(
        units, cols, keys, state, part
    )

    home = lax.all_to_all(grads.reshape(8, tokens, -1), "lane", 0, 0, tiled=True)

    def to_rows(array):
        return jnp.moveaxis(array, 0, 1).reshape(tokens, -1)

    grad_key = to_rows(home[:, :, 0:256])
    grad_query = to_rows(home[:, :, 256:512])
    grad_value = to_rows(home[:, :, 512:1024])
    grad_input = dot(grad_key, weight, NT).astype(BF16)

    terms = dot(gathered, grads[:, 0:256], TN).astype(BF16)
    group = DP + ("half",)
    terms = terms.reshape(lax.axis_size(group), -1, 256)
    terms = lax.all_to_all(terms, group, 0, 0, tiled=True)
    total = jnp.sum(terms.astype(F32), axis=0).astype(BF16)
    span = total.shape[0]
    spread = jnp.broadcast_to(total[None], (peers, span, 256))
    spread = lax.all_to_all(spread, SP, 0, 0, tiled=True)
    grad_weight = jnp.moveaxis(spread.reshape(2, 8, span, 256), 1, 2).reshape(2 * span, -1)
    return grad_query[None], grad_value[None], grad_input[None], grad_weight.astype(F32)


def solution(mesh):
    dp = mesh.shape["dp"]
    outer = (dp // 2, 2) if dp > 1 else (1, 1)
    finer = Mesh(mesh.devices.reshape(2, 8, *outer), SP + DP)
    part = P(DP, SP, None)
    return jax.shard_map(
        shards,
        mesh=finer,
        in_specs=(part, part, part, part, part, part, P(DP, None)),
        out_specs=(part, part, part, P(DP, None)),
        check_vma=False,
    )
```

```python
import jax
import jax.numpy as jnp
from jax import lax
from jax.experimental import pallas as pl
from jax.experimental.pallas import tpu as pltpu
from jax.sharding import Mesh
from jax.sharding import PartitionSpec as P


HEADS = 8
BLOCK = 128
TILE = 256
SP = ("half", "lane")
DP = ("dp_0", "dp_1")
F32 = jnp.float32
BF16 = jnp.bfloat16


def dot(a, b, dims, precision=None):
    return lax.dot_general(a, b, (dims, ((), ())), precision=precision, preferred_element_type=F32)


NN = ((1,), (0,))
NT = ((1,), (1,))
TN = ((0,), (0,))


def decay_kernel(lam_ref, half_ref, rows_ref, cols_ref):
    n = BLOCK
    row = lax.broadcasted_iota(jnp.int32, (n, n), 0)
    col = lax.broadcasted_iota(jnp.int32, (n, n), 1)
    lam = lam_ref[...]
    high = lax.Precision.HIGHEST
    upto = dot(lam, (row <= col).astype(F32), NN, high)
    before = dot(lam, (row < col).astype(F32), NN, high)
    since = dot(lam, (row >= col).astype(F32), NN, high)
    after = dot(lam, (row > col).astype(F32), NN, high)
    totals = [jnp.broadcast_to(upto[b : b + 1, n - 1 : n], (1, n)) for b in range(16)]
    loc0, suf1, rem0, pre1 = [], [], [], []
    for b in range(8):
        odd = b % 2 == 1
        loc0.append(upto[b : b + 1] + totals[b - 1] if odd else upto[b : b + 1])
        suf1.append(since[8 + b : 9 + b] if odd else since[8 + b : 9 + b] + totals[9 + b])
        rem0.append(after[b : b + 1] if odd else after[b : b + 1] + totals[b + 1])
        pre1.append(before[8 + b : 9 + b] + totals[7 + b] if odd else before[8 + b : 9 + b])
    tile0 = [totals[2 * t] + totals[2 * t + 1] for t in range(4)]
    tile1 = [totals[8 + 2 * t] + totals[9 + 2 * t] for t in range(4)]
    first = half_ref[...] == 0
    key_sum, query_sum = [], []
    for b in range(8):
        t = b // 2
        later0, later1 = sum(tile0[t + 1 :]), sum(tile1[t + 1 :])
        early0, early1 = sum(tile0[:t]), sum(tile1[:t])
        key_sum.append(jnp.where(first, rem0[b] + later0, pre1[b] + early1))
        query_sum.append(jnp.where(first, suf1[b] + later1, loc0[b] + early0))
    rows_ref[...] = jnp.concatenate(loc0 + suf1 + rem0 + pre1 + tile0 + tile1, axis=0)
    keys = jnp.exp(jnp.concatenate(key_sum, axis=0))
    queries = jnp.exp(jnp.concatenate(query_sum, axis=0)) * 0.0625
    stack = [jnp.concatenate(loc0 + suf1, axis=0), keys, queries, jnp.zeros((n - 32, n), F32)]
    cols_ref[...] = jnp.transpose(jnp.concatenate(stack, axis=0))


def tall(cols, base, block_pair=None):
    picks = range(8) if block_pair is None else (2 * block_pair, 2 * block_pair + 1)
    return jnp.concatenate([cols[:, base + b : base + b + 1] for b in picks], axis=0)


def wide(rows, base, t):
    return jnp.concatenate([rows[base + 2 * t : base + 2 * t + 1], rows[base + 2 * t + 1 : base + 2 * t + 2]], axis=1)


def boundary_kernel(units_ref, cols_ref, state_ref, keys_ref):
    cols = cols_ref[...]
    keys = (units_ref[:, 256:512].astype(F32) * tall(cols, 16)).astype(BF16)
    queries = (units_ref[:, 0:256].astype(F32) * tall(cols, 24)).astype(BF16)
    keys_ref[...] = keys
    state_ref[0] = dot(keys, units_ref[:, 512:1024], TN).astype(BF16)
    state_ref[1] = dot(queries, units_ref[:, 1024:1536], TN).astype(BF16)


def inside_kernel(units_ref, rows_ref, cols_ref, out_ref, s_ref, gs_ref):
    rows, cols = rows_ref[...], cols_ref[...]
    row = lax.broadcasted_iota(jnp.int32, (TILE, TILE), 0)
    col = lax.broadcasted_iota(jnp.int32, (TILE, TILE), 1)
    for i in range(4):
        at = pl.ds(i * TILE, TILE)
        query, grad = units_ref[at, 0:256], units_ref[at, 1024:1536]
        loc0, suf1 = tall(cols, 0, i), tall(cols, 8, i)
        for j in range(4):
            to = pl.ds(j * TILE, TILE)
            if i == j:
                spread = jnp.where(row >= col, loc0 - wide(rows, 0, i), suf1 - wide(rows, 8, i))
            elif i > j:
                along = wide(rows, 16, j)
                for t in range(j + 1, i):
                    along = along + jnp.concatenate([rows[32 + t : 33 + t]] * 2, axis=1)
                spread = loc0 + along
            else:
                along = wide(rows, 24, j)
                for t in range(i + 1, j):
                    along = along + jnp.concatenate([rows[36 + t : 37 + t]] * 2, axis=1)
                spread = suf1 + along
            weights = jnp.exp(spread) * 0.0625
            scores = dot(query, units_ref[to, 256:512], NT)
            grads = dot(grad, units_ref[to, 512:1024], NT)
            s_ref[at, to] = (scores * weights).astype(BF16)
            gs_ref[at, to] = (grads * weights).astype(BF16)
    out_ref[:, 0:256] = dot(gs_ref[...], units_ref[:, 0:256], TN)
    out_ref[:, 256:512] = dot(gs_ref[...], units_ref[:, 256:512], NN)
    out_ref[:, 512:1024] = dot(s_ref[...], units_ref[:, 1024:1536], TN)


def across_kernel(units_ref, cols_ref, keys_ref, state_ref, part_ref, out_ref):
    cols = cols_ref[...]
    memory, later = state_ref[0], state_ref[1]
    key_part = dot(units_ref[:, 512:1024], later, NT) * tall(cols, 16)
    out_ref[:, 0:256] = (part_ref[:, 0:256] + key_part).astype(BF16)
    query_part = dot(units_ref[:, 1024:1536], memory, NT) * tall(cols, 24)
    out_ref[:, 256:512] = (part_ref[:, 256:512] + query_part).astype(BF16)
    value_part = dot(keys_ref[...], later, NN)
    out_ref[:, 512:1024] = (part_ref[:, 512:1024] + value_part).astype(BF16)


def kernel(body, out_shape, flops, scratch=(), **grid):
    return pl.pallas_call(
        body,
        out_shape=out_shape,
        scratch_shapes=scratch,
        cost_estimate=pl.CostEstimate(flops=flops, bytes_accessed=4 << 20, transcendentals=0),
        compiler_params=pltpu.CompilerParams(vmem_limit_bytes=48 << 20),
        **grid,
    )


def shape(dims, dtype):
    return jax.ShapeDtypeStruct(dims, dtype)


def pack_kernel(query_ref, key_ref, value_ref, grad_ref, out_ref):
    out_ref[0, :, 0:256] = query_ref[...]
    out_ref[0, :, 256:512] = key_ref[...]
    out_ref[0, :, 512:1024] = value_ref[...]
    out_ref[0, :, 1024:1536] = grad_ref[...]


def by_head(width):
    return pl.BlockSpec((BLOCK, width), lambda h: (0, h))


def term_kernel(lane_ref, grads_ref, own_ref, before_ref, after_ref, far_ref, out_ref):
    lane = lane_ref[0]
    deep, y = lane // 4, lane % 4
    total = None
    for pair, step in ((own_ref, 0), (before_ref, 3), (after_ref, 1), (far_ref, 2)):
        for other in range(2):
            block = (deep ^ other) * 4 + (y + step) % 4
            grad = grads_ref[pl.ds(pl.multiple_of(block * BLOCK, BLOCK), BLOCK), 0:256]
            part = dot(pair[other], grad, TN)
            total = part if total is None else total + part
    out_ref[...] = total.astype(BF16)


def home_kernel(home_ref, weight_ref, query_ref, value_ref, input_ref, sum_ref):
    query_ref[...] = home_ref[0, :, 256:512]
    value_ref[...] = home_ref[0, :, 512:1024]
    part = dot(home_ref[0, :, 0:256], weight_ref[...], NT)
    first = pl.program_id(0) == 0

    @pl.when(first)
    def _():
        sum_ref[...] = part

    @pl.when(jnp.logical_not(first))
    def _():
        sum_ref[...] += part

    @pl.when(pl.program_id(0) == pl.num_programs(0) - 1)
    def _():
        input_ref[...] = sum_ref[...].astype(BF16)


def widen_kernel(in_ref, out_ref):
    out_ref[...] = in_ref[0].astype(F32)


def shards(layer_input, queries, key_vectors, values, cotangent, log_decay, key_weight):
    tokens = layer_input.shape[1]
    half = lax.axis_index("half")
    lane = lax.axis_index("lane")
    peers = lax.axis_size(SP)
    ring = lax.axis_size("dp_0")
    weight = lax.all_gather(key_weight, DP, tiled=True)

    decay = log_decay.reshape(2, 8, BLOCK)
    own = lane % 2
    near = lax.dynamic_index_in_dim(decay, own, 0, keepdims=False)
    far = lax.dynamic_index_in_dim(decay, 1 - own, 0, keepdims=False)
    near = lax.ppermute(near, SP, [(u, u % 2 * 8 + u // 2) for u in range(peers)])
    far = lax.ppermute(far, SP, [(u, (1 - u % 2) * 8 + u // 2) for u in range(peers)])
    lam = jnp.where(half == 0, jnp.concatenate([near, far]), jnp.concatenate([far, near]))
    rows, cols = kernel(decay_kernel, (shape((40, 128), F32), shape((128, 128), F32)), 1 << 20)(
        lam, jnp.full((1, 128), half, jnp.int32)
    )

    sent = kernel(
        pack_kernel,
        shape((8, tokens, 1536), BF16),
        1 << 20,
        grid=(HEADS,),
        in_specs=[by_head(256), by_head(256), by_head(512), by_head(512)],
        out_specs=pl.BlockSpec((1, tokens, 1536), lambda h: (h, 0, 0)),
    )(queries[0], key_vectors[0], values[0], cotangent[0])
    units = lax.all_to_all(sent, "lane", 0, 0, tiled=True).reshape(8 * tokens, -1)

    def lane_step(array, step):
        return lax.ppermute(
            array, "lane", [(i, i // 4 * 4 + (i + step) % 4) for i in range(8)]
        )

    across = lax.ppermute(layer_input, "lane", [(i, (i + 4) % 8) for i in range(8)])
    pair = jnp.concatenate([layer_input, across])
    pair, units = lax.optimization_barrier((pair, units))
    before, after = lane_step(pair, 1), lane_step(pair, 3)
    opposite = jnp.concatenate([lane_step(before[0:1], 1), lane_step(after[1:2], 3)])

    state, keys = kernel(
        boundary_kernel, (shape((2, 256, 512), BF16), shape((1024, 256), BF16)), 540 << 20
    )(units, cols)
    state = lax.ppermute(state, SP, [(u, (u + 8) % 16) for u in range(peers)])
    part = kernel(
        inside_kernel,
        shape((1024, 1024), F32),
        3760 << 20,
        (pltpu.VMEM((1024, 1024), BF16), pltpu.VMEM((1024, 1024), BF16)),
    )(units, rows, cols)
    grads = kernel(across_kernel, shape((1024, 1024), BF16), 800 << 20)(
        units, cols, keys, state, part
    )

    home = lax.all_to_all(grads.reshape(8, tokens, -1), "lane", 0, 0, tiled=True)
    grad_query, grad_value, grad_input = kernel(
        home_kernel,
        (shape((tokens, 2048), BF16), shape((tokens, 4096), BF16), shape((tokens, 2048), BF16)),
        1070 << 20,
        (pltpu.VMEM((tokens, 2048), F32),),
        grid=(HEADS,),
        in_specs=[
            pl.BlockSpec((1, tokens, 1024), lambda h: (h, 0, 0)),
            pl.BlockSpec((2048, 256), lambda h: (0, h)),
        ],
        out_specs=(by_head(256), by_head(512), pl.BlockSpec((tokens, 2048), lambda h: (0, 0))),
    )(home, weight)

    whole = pl.BlockSpec(memory_space=pltpu.VMEM)
    terms = kernel(
        term_kernel,
        shape((2048, 256), BF16),
        1070 << 20,
        in_specs=[pl.BlockSpec(memory_space=pltpu.SMEM)] + [whole] * 5,
        out_specs=whole,
    )(lane.reshape(1), grads, pair, before, after, opposite)

    core = lax.axis_index("dp_1")
    across_ring = lax.axis_index("dp_0")
    cores = lax.axis_size("dp_1")
    if cores == 2:
        terms = terms.reshape(ring, 2, -1, 256)
        mine = lax.dynamic_index_in_dim(terms, core, 1, keepdims=False)
        theirs = lax.dynamic_index_in_dim(terms, 1 - core, 1, keepdims=False)
        theirs = lax.ppermute(theirs, "dp_1", [(0, 1), (1, 0)])
        terms = (mine.astype(F32) + theirs.astype(F32)).astype(BF16)
        total = lax.dynamic_index_in_dim(terms, across_ring, 0, keepdims=False).astype(F32)
        for step in range(1, ring):
            piece = lax.dynamic_index_in_dim(terms, (across_ring + step) % ring, 0, keepdims=False)
            piece = lax.ppermute(piece, "dp_0", [(i, (i + step) % ring) for i in range(ring)])
            total = total + piece.astype(F32)
        terms = total.astype(BF16)
    terms = terms.reshape(2, -1, 256)
    mine = lax.dynamic_index_in_dim(terms, half, 0, keepdims=False)
    theirs = lax.dynamic_index_in_dim(terms, 1 - half, 0, keepdims=False)
    theirs = lax.ppermute(theirs, "half", [(0, 1), (1, 0)])
    total = (mine.astype(F32) + theirs.astype(F32)).astype(BF16)
    span = total.shape[0]
    spread = jnp.broadcast_to(total[None], (peers, span, 256))
    spread = lax.all_to_all(spread, SP, 0, 0, tiled=True)
    grad_weight = kernel(
        widen_kernel,
        shape((2 * span, 2048), F32),
        1 << 20,
        grid=(2, HEADS),
        in_specs=[pl.BlockSpec((1, span, 256), lambda s, h: (s * 8 + h, 0, 0))],
        out_specs=pl.BlockSpec((span, 256), lambda s, h: (s, h)),
    )(spread)
    return grad_query[None], grad_value[None], grad_input[None], grad_weight


def solution(mesh):
    dp = mesh.shape["dp"]
    outer = (dp // 2, 2) if dp > 1 else (1, 1)
    finer = Mesh(mesh.devices.reshape(2, 8, *outer), SP + DP)
    part = P(DP, SP, None)
    return jax.shard_map(
        shards,
        mesh=finer,
        in_specs=(part, part, part, part, part, part, P(DP, None)),
        out_specs=(part, part, part, P(DP, None)),
        check_vma=False,
    )
```

```python
import jax
import jax.numpy as jnp
from jax import lax
from jax.experimental import pallas as pl
from jax.experimental.pallas import tpu as pltpu
from jax.sharding import Mesh
from jax.sharding import PartitionSpec as P


HEADS = 8
BLOCK = 128
TILE = 256
SP = ("half", "lane")
DP = ("dp_0", "dp_1")
F32 = jnp.float32
BF16 = jnp.bfloat16


def dot(a, b, dims, precision=None):
    return lax.dot_general(a, b, (dims, ((), ())), precision=precision, preferred_element_type=F32)


NN = ((1,), (0,))
NT = ((1,), (1,))
TN = ((0,), (0,))


def decay_kernel(lam_ref, half_ref, rows_ref, tall_ref):
    n = BLOCK
    row = lax.broadcasted_iota(jnp.int32, (n, n), 0)
    col = lax.broadcasted_iota(jnp.int32, (n, n), 1)
    lam = lam_ref[...]
    high = lax.Precision.HIGHEST
    upto = dot(lam, (row <= col).astype(F32), NN, high)
    before = dot(lam, (row < col).astype(F32), NN, high)
    since = dot(lam, (row >= col).astype(F32), NN, high)
    after = dot(lam, (row > col).astype(F32), NN, high)
    totals = [jnp.broadcast_to(upto[b : b + 1, n - 1 : n], (1, n)) for b in range(16)]
    loc0, suf1, rem0, pre1 = [], [], [], []
    for b in range(8):
        odd = b % 2 == 1
        loc0.append(upto[b : b + 1] + totals[b - 1] if odd else upto[b : b + 1])
        suf1.append(since[8 + b : 9 + b] if odd else since[8 + b : 9 + b] + totals[9 + b])
        rem0.append(after[b : b + 1] if odd else after[b : b + 1] + totals[b + 1])
        pre1.append(before[8 + b : 9 + b] + totals[7 + b] if odd else before[8 + b : 9 + b])
    tile0 = [totals[2 * t] + totals[2 * t + 1] for t in range(4)]
    tile1 = [totals[8 + 2 * t] + totals[9 + 2 * t] for t in range(4)]
    first = half_ref[...] == 0
    key_sum, query_sum = [], []
    for b in range(8):
        t = b // 2
        later0, later1 = sum(tile0[t + 1 :]), sum(tile1[t + 1 :])
        early0, early1 = sum(tile0[:t]), sum(tile1[:t])
        key_sum.append(jnp.where(first, rem0[b] + later0, pre1[b] + early1))
        query_sum.append(jnp.where(first, suf1[b] + later1, loc0[b] + early0))
    rows_ref[...] = jnp.concatenate(loc0 + suf1 + rem0 + pre1 + tile0 + tile1, axis=0)
    keys = jnp.exp(jnp.concatenate(key_sum, axis=0))
    queries = jnp.exp(jnp.concatenate(query_sum, axis=0)) * 0.0625
    stack = [jnp.concatenate(loc0 + suf1, axis=0), keys, queries, jnp.zeros((n - 32, n), F32)]
    cols = jnp.transpose(jnp.concatenate(stack, axis=0))
    for b in range(8):
        picks = [cols[:, v * 8 + b : v * 8 + b + 1] for v in range(4)]
        tall_ref[b * n : b * n + n, :] = jnp.concatenate(picks, axis=1)


def wide(rows, base, t):
    return jnp.concatenate([rows[base + 2 * t : base + 2 * t + 1], rows[base + 2 * t + 1 : base + 2 * t + 2]], axis=1)


def boundary_kernel(units_ref, tall_ref, state_ref):
    keys = (units_ref[:, 256:512].astype(F32) * tall_ref[:, 2:3]).astype(BF16)
    queries = (units_ref[:, 0:256].astype(F32) * tall_ref[:, 3:4]).astype(BF16)
    state_ref[0] = dot(keys, units_ref[:, 512:1024], TN).astype(BF16)
    state_ref[1] = dot(queries, units_ref[:, 1024:1536], TN).astype(BF16)


def inside_kernel(units_ref, rows_ref, tall_ref, out_ref, s_ref, gs_ref):
    rows = rows_ref[...]
    row = lax.broadcasted_iota(jnp.int32, (TILE, TILE), 0)
    col = lax.broadcasted_iota(jnp.int32, (TILE, TILE), 1)
    for i in range(4):
        at = pl.ds(i * TILE, TILE)
        query, grad = units_ref[at, 0:256], units_ref[at, 1024:1536]
        loc0, suf1 = tall_ref[at, 0:1], tall_ref[at, 1:2]
        for j in range(4):
            to = pl.ds(j * TILE, TILE)
            if i == j:
                spread = jnp.where(row >= col, loc0 - wide(rows, 0, i), suf1 - wide(rows, 8, i))
            elif i > j:
                along = wide(rows, 16, j)
                for t in range(j + 1, i):
                    along = along + jnp.concatenate([rows[32 + t : 33 + t]] * 2, axis=1)
                spread = loc0 + along
            else:
                along = wide(rows, 24, j)
                for t in range(i + 1, j):
                    along = along + jnp.concatenate([rows[36 + t : 37 + t]] * 2, axis=1)
                spread = suf1 + along
            weights = jnp.exp(spread) * 0.0625
            scores = dot(query, units_ref[to, 256:512], NT)
            grads = dot(grad, units_ref[to, 512:1024], NT)
            s_ref[at, to] = (scores * weights).astype(BF16)
            gs_ref[at, to] = (grads * weights).astype(BF16)
    out_ref[:, 0:256] = dot(gs_ref[...], units_ref[:, 0:256], TN).astype(BF16)
    out_ref[:, 256:512] = dot(gs_ref[...], units_ref[:, 256:512], NN).astype(BF16)
    out_ref[:, 512:1024] = dot(s_ref[...], units_ref[:, 1024:1536], TN).astype(BF16)


def across_kernel(units_ref, tall_ref, state_ref, part_ref, out_ref):
    memory, later = state_ref[0], state_ref[1]
    keys = (units_ref[:, 256:512].astype(F32) * tall_ref[:, 2:3]).astype(BF16)
    part = dot(units_ref[:, 512:1024], later, NT) * tall_ref[:, 2:3]
    out_ref[:, 0:256] = (part_ref[:, 0:256].astype(F32) + part).astype(BF16)
    part = dot(units_ref[:, 1024:1536], memory, NT) * tall_ref[:, 3:4]
    out_ref[:, 256:512] = (part_ref[:, 256:512].astype(F32) + part).astype(BF16)
    part = dot(keys, later, NN)
    out_ref[:, 512:1024] = (part_ref[:, 512:1024].astype(F32) + part).astype(BF16)


def kernel(body, out_shape, flops, scratch=(), **grid):
    return pl.pallas_call(
        body,
        out_shape=out_shape,
        scratch_shapes=scratch,
        cost_estimate=pl.CostEstimate(flops=flops, bytes_accessed=4 << 20, transcendentals=0),
        compiler_params=pltpu.CompilerParams(vmem_limit_bytes=24 << 20),
        **grid,
    )


def in_hbm(array):
    return pltpu.with_memory_space_constraint(array, pltpu.HBM)


def shape(dims, dtype):
    return jax.ShapeDtypeStruct(dims, dtype)


def pack_kernel(query_ref, key_ref, value_ref, grad_ref, out_ref, sems):
    copies, at = [], 0
    for source in (query_ref, key_ref, value_ref, grad_ref):
        width = source.shape[1] // HEADS
        for h in range(HEADS):
            copies.append(
                pltpu.make_async_copy(
                    source.at[:, pl.ds(h * width, width)],
                    out_ref.at[h, :, pl.ds(at, width)],
                    sems.at[len(copies)],
                )
            )
        at += width
    for copy in copies:
        copy.start()
    for copy in copies:
        copy.wait()


STEPS = ((0, 0), (1, 0), (0, 3), (0, 1), (1, 3), (1, 1), (0, 2), (1, 2))


def term_kernel(lane_ref, grads_ref, *refs):
    lane = lane_ref[0]
    deep, y = lane // 4, lane % 4
    total = None
    for piece, (other, step) in zip(refs[:-1], STEPS, strict=True):
        block = (deep ^ other) * 4 + (y + step) % 4
        grad = grads_ref[pl.ds(pl.multiple_of(block * BLOCK, BLOCK), BLOCK), :]
        part = dot(piece[0], grad, TN)
        total = part if total is None else total + part
    refs[-1][...] = total.astype(BF16)


def home_kernel(owner_ref, home_ref, *refs):
    weights, (query_ref, value_ref, input_ref, key_ref) = refs[:-4], refs[-4:]
    for h in range(HEADS):
        key_ref[:, h * 256 : h * 256 + 256] = home_ref[h, :, 0:256]
        query_ref[:, h * 256 : h * 256 + 256] = home_ref[h, :, 256:512]
        value_ref[:, h * 512 : h * 512 + 512] = home_ref[h, :, 512:1024]
    for k, weight in enumerate(weights):
        span = weight.shape[0]
        at = pl.multiple_of(owner_ref[k] * span, span)
        input_ref[:, pl.ds(at, span)] = dot(key_ref[...], weight[...], NT).astype(BF16)


def widen_kernel(in_ref, out_ref):
    for s in range(2):
        for h in range(2):
            span = in_ref.shape[2]
            out_ref[s * span : s * span + span, h * 256 : h * 256 + 256] = in_ref[s, h].astype(F32)


def shards(layer_input, queries, key_vectors, values, cotangent, log_decay, key_weight):
    tokens = layer_input.shape[1]
    half = lax.axis_index("half")
    lane = lax.axis_index("lane")
    peers = lax.axis_size(SP)
    ring = lax.axis_size("dp_0")
    cores = lax.axis_size("dp_1")
    core, turn = lax.axis_index("dp_1"), lax.axis_index("dp_0")

    decay = log_decay.reshape(2, 8, BLOCK)
    own = lane % 2
    near = lax.dynamic_index_in_dim(decay, own, 0, keepdims=False)
    far = lax.dynamic_index_in_dim(decay, 1 - own, 0, keepdims=False)
    near = lax.ppermute(near, SP, [(u, u % 2 * 8 + u // 2) for u in range(peers)])
    far = lax.ppermute(far, SP, [(u, (1 - u % 2) * 8 + u // 2) for u in range(peers)])
    deep = lax.ppermute(layer_input, "lane", [(i, (i + 4) % 8) for i in range(8)])
    lam = jnp.where(half == 0, jnp.concatenate([near, far]), jnp.concatenate([far, near]))
    rows, tall = kernel(decay_kernel, (shape((40, 128), F32), pltpu.HBM((1024, 4), F32)), 1 << 20)(
        lam, jnp.full((1, 128), half, jnp.int32)
    )

    outside = pl.BlockSpec(memory_space=pltpu.HBM)
    whole = pl.BlockSpec(memory_space=pltpu.VMEM)
    scalars = pl.BlockSpec(memory_space=pltpu.SMEM)
    sent = kernel(
        pack_kernel,
        pltpu.HBM((8, tokens, 1536), BF16),
        1 << 20,
        (pltpu.SemaphoreType.DMA((32,)),),
        in_specs=[outside] * 4,
        out_specs=outside,
    )(*[in_hbm(a[0]) for a in (queries, key_vectors, values, cotangent)])
    units = lax.all_to_all(sent, "lane", 0, 0, tiled=True).reshape(8 * tokens, -1)

    def lane_step(array, step):
        return lax.ppermute(
            array, "lane", [(i, i // 4 * 4 + (i + step) % 4) for i in range(8)]
        )

    weights, owners = [key_weight], [turn * cores + core]
    for step in range(1, ring):
        moves = [(i, (i + step) % ring) for i in range(ring)]
        weights.append(lax.ppermute(key_weight, "dp_0", moves))
        owners.append((turn - step) % ring * cores + core)
    if cores == 2:
        weights += [lax.ppermute(w, "dp_1", [(0, 1), (1, 0)]) for w in weights]
        owners += [o + 1 - 2 * core for o in owners]

    own, deep, units = lax.optimization_barrier((layer_input, deep, units))
    own_before, own_after = lane_step(own, 1), lane_step(own, 3)
    deep_before, deep_after = lane_step(deep, 1), lane_step(deep, 3)
    own_last, deep_last = lane_step(own_before, 1), lane_step(deep_after, 3)

    state = kernel(boundary_kernel, pltpu.HBM((2, 256, 512), BF16), 540 << 20)(units, tall)
    state = lax.ppermute(state, SP, [(u, (u + 8) % 16) for u in range(peers)])
    part = kernel(
        inside_kernel,
        pltpu.HBM((1024, 1024), BF16),
        3760 << 20,
        (pltpu.VMEM((1024, 1024), BF16), pltpu.VMEM((1024, 1024), BF16)),
    )(units, rows, tall)

    def by_tile(width):
        return pl.BlockSpec((TILE, width), lambda i: (i, 0))

    grads = kernel(
        across_kernel,
        pltpu.HBM((1024, 1024), BF16),
        800 << 20,
        grid=(4,),
        in_specs=[
            by_tile(1536),
            by_tile(4),
            pl.BlockSpec((2, 256, 512), lambda i: (0, 0, 0)),
            by_tile(1024),
        ],
        out_specs=by_tile(1024),
    )(units, tall, state, in_hbm(part))

    home = lax.all_to_all(grads.reshape(8, tokens, -1), "lane", 0, 0, tiled=True)
    grad_query, grad_value, grad_input = kernel(
        home_kernel,
        (shape((tokens, 2048), BF16), shape((tokens, 4096), BF16), shape((tokens, 2048), BF16)),
        1070 << 20,
        (pltpu.VMEM((tokens, 2048), BF16),),
        in_specs=[scalars] + [whole] * (1 + len(weights)),
        out_specs=(whole, whole, whole),
    )(jnp.stack(owners), home, *weights)

    terms = kernel(
        term_kernel,
        shape((2048, 256), BF16),
        1070 << 20,
        grid=(1,),
        in_specs=[scalars, pl.BlockSpec((1024, 256), lambda i: (0, 0))] + [whole] * 8,
        out_specs=whole,
    )(
        lane.reshape(1),
        in_hbm(grads),
        own,
        deep,
        own_before,
        own_after,
        deep_before,
        deep_after,
        own_last,
        deep_last,
    )

    if cores == 2:
        terms = terms.reshape(ring, 2, -1, 256)
        mine = lax.dynamic_index_in_dim(terms, core, 1, keepdims=False)
        theirs = lax.dynamic_index_in_dim(terms, 1 - core, 1, keepdims=False)
        theirs = lax.ppermute(theirs, "dp_1", [(0, 1), (1, 0)])
        terms = (mine.astype(F32) + theirs.astype(F32)).astype(BF16)
        total = lax.dynamic_index_in_dim(terms, turn, 0, keepdims=False).astype(F32)
        for step in range(1, ring):
            piece = lax.dynamic_index_in_dim(terms, (turn + step) % ring, 0, keepdims=False)
            piece = lax.ppermute(piece, "dp_0", [(i, (i + step) % ring) for i in range(ring)])
            total = total + piece.astype(F32)
        terms = total.astype(BF16)
    terms = terms.reshape(2, -1, 256)
    mine = lax.dynamic_index_in_dim(terms, half, 0, keepdims=False)
    theirs = lax.dynamic_index_in_dim(terms, 1 - half, 0, keepdims=False)
    theirs = lax.ppermute(theirs, "half", [(0, 1), (1, 0)])
    total = (mine.astype(F32) + theirs.astype(F32)).astype(BF16)
    span = total.shape[0]
    spread = jnp.broadcast_to(total[None], (peers, span, 256))
    spread = lax.all_to_all(spread, SP, 0, 0, tiled=True)
    grad_weight = kernel(
        widen_kernel,
        shape((2 * span, 2048), F32),
        1 << 20,
        grid=(4,),
        in_specs=[pl.BlockSpec((2, 2, span, 256), lambda h: (0, h, 0, 0))],
        out_specs=pl.BlockSpec((2 * span, 512), lambda h: (0, h)),
    )(spread.reshape(2, 8, span, 256))
    return grad_query[None], grad_value[None], grad_input[None], grad_weight


def solution(mesh):
    dp = mesh.shape["dp"]
    outer = (dp // 2, 2) if dp > 1 else (1, 1)
    finer = Mesh(mesh.devices.reshape(2, 8, *outer), SP + DP)
    part = P(DP, SP, None)
    return jax.shard_map(
        shards,
        mesh=finer,
        in_specs=(part, part, part, part, part, part, P(DP, None)),
        out_specs=(part, part, part, P(DP, None)),
        check_vma=False,
    )
```

```python
import jax
import jax.numpy as jnp
from jax import lax
from jax.experimental import pallas as pl
from jax.experimental.pallas import tpu as pltpu
from jax.sharding import Mesh
from jax.sharding import PartitionSpec as P


HEADS = 8
BLOCK = 128
TILE = 256
SP = ("half", "lane")
DP = ("dp_0", "dp_1")
F32 = jnp.float32
BF16 = jnp.bfloat16


def dot(a, b, dims, precision=None):
    return lax.dot_general(a, b, (dims, ((), ())), precision=precision, preferred_element_type=F32)


NN = ((1,), (0,))
NT = ((1,), (1,))
TN = ((0,), (0,))


def decay_kernel(lam_ref, half_ref, rows_ref, tall_ref):
    n = BLOCK
    row = lax.broadcasted_iota(jnp.int32, (n, n), 0)
    col = lax.broadcasted_iota(jnp.int32, (n, n), 1)
    lam = lam_ref[...]
    high = lax.Precision.HIGHEST
    upto = dot(lam, (row <= col).astype(F32), NN, high)
    before = dot(lam, (row < col).astype(F32), NN, high)
    since = dot(lam, (row >= col).astype(F32), NN, high)
    after = dot(lam, (row > col).astype(F32), NN, high)
    totals = [jnp.broadcast_to(upto[b : b + 1, n - 1 : n], (1, n)) for b in range(16)]
    loc0, suf1, rem0, pre1 = [], [], [], []
    for b in range(8):
        odd = b % 2 == 1
        loc0.append(upto[b : b + 1] + totals[b - 1] if odd else upto[b : b + 1])
        suf1.append(since[8 + b : 9 + b] if odd else since[8 + b : 9 + b] + totals[9 + b])
        rem0.append(after[b : b + 1] if odd else after[b : b + 1] + totals[b + 1])
        pre1.append(before[8 + b : 9 + b] + totals[7 + b] if odd else before[8 + b : 9 + b])
    tile0 = [totals[2 * t] + totals[2 * t + 1] for t in range(4)]
    tile1 = [totals[8 + 2 * t] + totals[9 + 2 * t] for t in range(4)]
    first = half_ref[...] == 0
    key_sum, query_sum = [], []
    for b in range(8):
        t = b // 2
        later0, later1 = sum(tile0[t + 1 :]), sum(tile1[t + 1 :])
        early0, early1 = sum(tile0[:t]), sum(tile1[:t])
        key_sum.append(jnp.where(first, rem0[b] + later0, pre1[b] + early1))
        query_sum.append(jnp.where(first, suf1[b] + later1, loc0[b] + early0))
    rows_ref[...] = jnp.concatenate(loc0 + suf1 + rem0 + pre1 + tile0 + tile1, axis=0)
    keys = jnp.exp(jnp.concatenate(key_sum, axis=0))
    queries = jnp.exp(jnp.concatenate(query_sum, axis=0)) * 0.0625
    stack = [jnp.concatenate(loc0 + suf1, axis=0), keys, queries, jnp.zeros((n - 32, n), F32)]
    cols = jnp.transpose(jnp.concatenate(stack, axis=0))
    for b in range(8):
        picks = [cols[:, v * 8 + b : v * 8 + b + 1] for v in range(4)]
        tall_ref[b * n : b * n + n, :] = jnp.concatenate(picks, axis=1)


def wide(rows, base, t):
    return jnp.concatenate([rows[base + 2 * t : base + 2 * t + 1], rows[base + 2 * t + 1 : base + 2 * t + 2]], axis=1)


def boundary_kernel(units_ref, tall_ref, state_ref):
    keys = (units_ref[:, 256:512].astype(F32) * tall_ref[:, 2:3]).astype(BF16)
    queries = (units_ref[:, 0:256].astype(F32) * tall_ref[:, 3:4]).astype(BF16)
    state_ref[0] = dot(keys, units_ref[:, 512:1024], TN).astype(BF16)
    state_ref[1] = dot(queries, units_ref[:, 1024:1536], TN).astype(BF16)


def inside_kernel(units_ref, rows_ref, tall_ref, out_ref, s_ref, gs_ref):
    rows = rows_ref[...]
    row = lax.broadcasted_iota(jnp.int32, (TILE, TILE), 0)
    col = lax.broadcasted_iota(jnp.int32, (TILE, TILE), 1)
    for i in range(4):
        at = pl.ds(i * TILE, TILE)
        query, grad = units_ref[at, 0:256], units_ref[at, 1024:1536]
        loc0, suf1 = tall_ref[at, 0:1], tall_ref[at, 1:2]
        for j in range(4):
            to = pl.ds(j * TILE, TILE)
            if i == j:
                spread = jnp.where(row >= col, loc0 - wide(rows, 0, i), suf1 - wide(rows, 8, i))
            elif i > j:
                along = wide(rows, 16, j)
                for t in range(j + 1, i):
                    along = along + jnp.concatenate([rows[32 + t : 33 + t]] * 2, axis=1)
                spread = loc0 + along
            else:
                along = wide(rows, 24, j)
                for t in range(i + 1, j):
                    along = along + jnp.concatenate([rows[36 + t : 37 + t]] * 2, axis=1)
                spread = suf1 + along
            weights = jnp.exp(spread) * 0.0625
            scores = dot(query, units_ref[to, 256:512], NT)
            grads = dot(grad, units_ref[to, 512:1024], NT)
            s_ref[at, to] = (scores * weights).astype(BF16)
            gs_ref[at, to] = (grads * weights).astype(BF16)
    out_ref[:, 0:256] = dot(gs_ref[...], units_ref[:, 0:256], TN).astype(BF16)
    out_ref[:, 256:512] = dot(gs_ref[...], units_ref[:, 256:512], NN).astype(BF16)
    out_ref[:, 512:1024] = dot(s_ref[...], units_ref[:, 1024:1536], TN).astype(BF16)


def across_kernel(units_ref, tall_ref, state_ref, part_ref, out_ref):
    memory, later = state_ref[0], state_ref[1]
    keys = (units_ref[:, 256:512].astype(F32) * tall_ref[:, 2:3]).astype(BF16)
    part = dot(units_ref[:, 512:1024], later, NT) * tall_ref[:, 2:3]
    out_ref[:, 0:256] = (part_ref[:, 0:256].astype(F32) + part).astype(BF16)
    part = dot(units_ref[:, 1024:1536], memory, NT) * tall_ref[:, 3:4]
    out_ref[:, 256:512] = (part_ref[:, 256:512].astype(F32) + part).astype(BF16)
    part = dot(keys, later, NN)
    out_ref[:, 512:1024] = (part_ref[:, 512:1024].astype(F32) + part).astype(BF16)


def kernel(body, out_shape, flops, scratch=(), **grid):
    return pl.pallas_call(
        body,
        out_shape=out_shape,
        scratch_shapes=scratch,
        cost_estimate=pl.CostEstimate(flops=flops, bytes_accessed=4 << 20, transcendentals=0),
        compiler_params=pltpu.CompilerParams(vmem_limit_bytes=24 << 20),
        **grid,
    )


def in_hbm(array):
    return pltpu.with_memory_space_constraint(array, pltpu.HBM)


def shape(dims, dtype):
    return jax.ShapeDtypeStruct(dims, dtype)


def pack_kernel(half_ref, query_ref, key_ref, value_ref, grad_ref, out_ref):
    del half_ref
    out_ref[0, :, 0:256] = query_ref[...]
    out_ref[0, :, 256:512] = key_ref[...]
    out_ref[0, :, 512:1024] = value_ref[...]
    out_ref[0, :, 1024:1536] = grad_ref[...]


def pack(half, arrays):
    def columns(width):
        return pl.BlockSpec((BLOCK, width), lambda h, half: (0, (h + 4 * half[0]) & 7))

    return pl.pallas_call(
        pack_kernel,
        out_shape=pltpu.HBM((HEADS, BLOCK, 1536), BF16),
        grid_spec=pltpu.PrefetchScalarGridSpec(
            num_scalar_prefetch=1,
            grid=(HEADS,),
            in_specs=[columns(a.shape[1] // HEADS) for a in arrays],
            out_specs=pl.BlockSpec((1, BLOCK, 1536), lambda h, half: (h, 0, 0)),
        ),
        cost_estimate=pl.CostEstimate(flops=1 << 20, bytes_accessed=6 << 20, transcendentals=0),
        compiler_params=pltpu.CompilerParams(vmem_limit_bytes=16 << 20),
    )(half.reshape(1), *[in_hbm(a) for a in arrays])


def worker(half, head):
    return half * 8 + (head + 4 * half) % 8


STEPS = ((0, 0), (1, 0), (0, 3), (0, 1), (1, 3), (1, 1), (0, 2), (1, 2))


def term_kernel(lane_ref, grads_ref, *refs):
    lane = lane_ref[0]
    deep, y = lane // 4, lane % 4
    total = None
    for piece, (other, step) in zip(refs[:-1], STEPS, strict=True):
        block = (deep ^ other) * 4 + (y + step) % 4
        grad = grads_ref[pl.ds(pl.multiple_of(block * BLOCK, BLOCK), BLOCK), :]
        part = dot(piece[0], grad, TN)
        total = part if total is None else total + part
    refs[-1][...] = total.astype(BF16)


def home_kernel(half_ref, owner_ref, home_ref, *refs):
    weights, (query_ref, value_ref, input_ref, key_ref) = refs[:-4], refs[-4:]
    for h in range(HEADS):
        lane = (h + 4 * half_ref[0]) & 7
        key_ref[:, h * 256 : h * 256 + 256] = home_ref[lane, :, 0:256]
        query_ref[:, h * 256 : h * 256 + 256] = home_ref[lane, :, 256:512]
        value_ref[:, h * 512 : h * 512 + 512] = home_ref[lane, :, 512:1024]
    for k, weight in enumerate(weights):
        span = weight.shape[0]
        at = pl.multiple_of(owner_ref[k] * span, span)
        input_ref[:, pl.ds(at, span)] = dot(key_ref[...], weight[...], NT).astype(BF16)


def widen_kernel(first_ref, second_ref, out_ref):
    span = first_ref.shape[2]
    for s, ref in enumerate((first_ref, second_ref)):
        for h in range(2):
            out_ref[s * span : s * span + span, h * 256 : h * 256 + 256] = ref[0, h].astype(F32)


def shards(layer_input, queries, key_vectors, values, cotangent, log_decay, key_weight):
    tokens = layer_input.shape[1]
    half = lax.axis_index("half")
    lane = lax.axis_index("lane")
    peers = lax.axis_size(SP)
    ring = lax.axis_size("dp_0")
    cores = lax.axis_size("dp_1")
    core, turn = lax.axis_index("dp_1"), lax.axis_index("dp_0")

    decay = log_decay.reshape(2, 8, BLOCK)
    own = lane % 2
    near = lax.dynamic_index_in_dim(decay, own, 0, keepdims=False)
    far = lax.dynamic_index_in_dim(decay, 1 - own, 0, keepdims=False)
    near = lax.ppermute(near, SP, [(u, worker(u % 2, u // 2)) for u in range(peers)])
    far = lax.ppermute(far, SP, [(u, worker(1 - u % 2, u // 2)) for u in range(peers)])
    deep = lax.ppermute(layer_input, "lane", [(i, (i + 4) % 8) for i in range(8)])
    lam = jnp.where(half == 0, jnp.concatenate([near, far]), jnp.concatenate([far, near]))
    rows, tall = kernel(decay_kernel, (shape((40, 128), F32), pltpu.HBM((1024, 4), F32)), 1 << 20)(
        lam, jnp.full((1, 128), half, jnp.int32)
    )

    whole = pl.BlockSpec(memory_space=pltpu.VMEM)
    scalars = pl.BlockSpec(memory_space=pltpu.SMEM)
    sent = pack(half, [a[0] for a in (queries, key_vectors, values, cotangent)])
    units = lax.all_to_all(sent, "lane", 0, 0, tiled=True).reshape(8 * tokens, -1)

    def lane_step(array, step):
        return lax.ppermute(
            array, "lane", [(i, i // 4 * 4 + (i + step) % 4) for i in range(8)]
        )

    weights, owners = [key_weight], [turn * cores + core]
    for step in range(1, ring):
        moves = [(i, (i + step) % ring) for i in range(ring)]
        weights.append(lax.ppermute(key_weight, "dp_0", moves))
        owners.append((turn - step) % ring * cores + core)
    if cores == 2:
        weights += [lax.ppermute(w, "dp_1", [(0, 1), (1, 0)]) for w in weights]
        owners += [o + 1 - 2 * core for o in owners]

    own = layer_input
    own_before, own_after = lane_step(own, 1), lane_step(own, 3)
    deep_before, deep_after = lane_step(deep, 1), lane_step(deep, 3)
    own_last, deep_last = lane_step(own_before, 1), lane_step(deep_after, 3)

    state = kernel(boundary_kernel, pltpu.HBM((2, 256, 512), BF16), 540 << 20)(units, tall)
    state = lax.ppermute(state, SP, [(u, u ^ 12) for u in range(peers)])
    part = kernel(
        inside_kernel,
        pltpu.HBM((1024, 1024), BF16),
        3760 << 20,
        (pltpu.VMEM((1024, 1024), BF16), pltpu.VMEM((1024, 1024), BF16)),
    )(units, rows, tall)

    def by_tile(width):
        return pl.BlockSpec((TILE, width), lambda i: (i, 0))

    grads = kernel(
        across_kernel,
        pltpu.HBM((1024, 1024), BF16),
        800 << 20,
        grid=(4,),
        in_specs=[
            by_tile(1536),
            by_tile(4),
            pl.BlockSpec((2, 256, 512), lambda i: (0, 0, 0)),
            by_tile(1024),
        ],
        out_specs=by_tile(1024),
    )(units, tall, state, in_hbm(part))

    home = lax.all_to_all(grads.reshape(8, tokens, -1), "lane", 0, 0, tiled=True)
    grad_query, grad_value, grad_input = kernel(
        home_kernel,
        (shape((tokens, 2048), BF16), shape((tokens, 4096), BF16), shape((tokens, 2048), BF16)),
        1070 << 20,
        (pltpu.VMEM((tokens, 2048), BF16),),
        in_specs=[scalars] * 2 + [whole] * (1 + len(weights)),
        out_specs=(whole, whole, whole),
    )(half.reshape(1), jnp.stack(owners), home, *weights)

    terms = kernel(
        term_kernel,
        shape((2048, 256), BF16),
        1070 << 20,
        grid=(1,),
        in_specs=[scalars, pl.BlockSpec((1024, 256), lambda i: (0, 0))] + [whole] * 8,
        out_specs=whole,
    )(
        lane.reshape(1),
        in_hbm(grads),
        own,
        deep,
        own_before,
        own_after,
        deep_before,
        deep_after,
        own_last,
        deep_last,
    )

    if cores == 2:
        terms = terms.reshape(ring, 2, -1, 256)
        mine = lax.dynamic_index_in_dim(terms, core, 1, keepdims=False)
        theirs = lax.dynamic_index_in_dim(terms, 1 - core, 1, keepdims=False)
        theirs = lax.ppermute(theirs, "dp_1", [(0, 1), (1, 0)])
        terms = (mine.astype(F32) + theirs.astype(F32)).astype(BF16)
        total = lax.dynamic_index_in_dim(terms, turn, 0, keepdims=False).astype(F32)
        for step in range(1, ring):
            piece = lax.dynamic_index_in_dim(terms, (turn + step) % ring, 0, keepdims=False)
            piece = lax.ppermute(piece, "dp_0", [(i, (i + step) % ring) for i in range(ring)])
            total = total + piece.astype(F32)
        terms = total.astype(BF16)
    terms = terms.reshape(2, -1, 256)
    mine = lax.dynamic_index_in_dim(terms, half, 0, keepdims=False)
    theirs = lax.dynamic_index_in_dim(terms, 1 - half, 0, keepdims=False)
    theirs = lax.ppermute(theirs, SP, [(u, u ^ 12) for u in range(peers)])
    total = (mine.astype(F32) + theirs.astype(F32)).astype(BF16)
    span = total.shape[0]
    spread = jnp.broadcast_to(total[None], (peers, span, 256))
    spread = lax.all_to_all(spread, SP, 0, 0, tiled=True)
    grad_weight = kernel(
        widen_kernel,
        shape((2 * span, 2048), F32),
        1 << 20,
        grid=(4,),
        in_specs=[
            pl.BlockSpec((1, 2, span, 256), lambda h: (0, h, 0, 0)),
            pl.BlockSpec((1, 2, span, 256), lambda h: (1, (h + 2) & 3, 0, 0)),
        ],
        out_specs=pl.BlockSpec((2 * span, 512), lambda h: (0, h)),
    )(*[spread.reshape(2, 8, span, 256)] * 2)
    return grad_query[None], grad_value[None], grad_input[None], grad_weight


def solution(mesh):
    dp = mesh.shape["dp"]
    outer = (dp // 2, 2) if dp > 1 else (1, 1)
    finer = Mesh(mesh.devices.reshape(2, 8, *outer), SP + DP)
    part = P(DP, SP, None)
    return jax.shard_map(
        shards,
        mesh=finer,
        in_specs=(part, part, part, part, part, part, P(DP, None)),
        out_specs=(part, part, part, P(DP, None)),
        check_vma=False,
    )
```

```python
import jax
import jax.numpy as jnp
from jax import lax
from jax.experimental import pallas as pl
from jax.experimental.pallas import tpu as pltpu
from jax.sharding import Mesh
from jax.sharding import PartitionSpec as P


HEADS = 8
BLOCK = 128
TILE = 256
SP = ("half", "lane")
DP = ("dp_0", "dp_1")
F32 = jnp.float32
BF16 = jnp.bfloat16


def dot(a, b, dims, precision=None):
    return lax.dot_general(a, b, (dims, ((), ())), precision=precision, preferred_element_type=F32)


NN = ((1,), (0,))
NT = ((1,), (1,))
TN = ((0,), (0,))


def decay_kernel(lam_ref, half_ref, rows_ref, factors_ref):
    n = BLOCK
    row = lax.broadcasted_iota(jnp.int32, (n, n), 0)
    col = lax.broadcasted_iota(jnp.int32, (n, n), 1)
    lam = lam_ref[...]
    high = lax.Precision.HIGHEST
    upto = dot(lam, (row <= col).astype(F32), NN, high)
    before = dot(lam, (row < col).astype(F32), NN, high)
    since = dot(lam, (row >= col).astype(F32), NN, high)
    after = dot(lam, (row > col).astype(F32), NN, high)
    totals = [jnp.broadcast_to(upto[b : b + 1, n - 1 : n], (1, n)) for b in range(16)]
    loc0, suf1, rem0, pre1 = [], [], [], []
    for b in range(8):
        odd = b % 2 == 1
        loc0.append(upto[b : b + 1] + totals[b - 1] if odd else upto[b : b + 1])
        suf1.append(since[8 + b : 9 + b] if odd else since[8 + b : 9 + b] + totals[9 + b])
        rem0.append(after[b : b + 1] if odd else after[b : b + 1] + totals[b + 1])
        pre1.append(before[8 + b : 9 + b] + totals[7 + b] if odd else before[8 + b : 9 + b])
    tile0 = [totals[2 * t] + totals[2 * t + 1] for t in range(4)]
    tile1 = [totals[8 + 2 * t] + totals[9 + 2 * t] for t in range(4)]
    first = half_ref[...] == 0
    key_sum, query_sum = [], []
    for b in range(8):
        t = b // 2
        later0, later1 = sum(tile0[t + 1 :]), sum(tile1[t + 1 :])
        early0, early1 = sum(tile0[:t]), sum(tile1[:t])
        key_sum.append(jnp.where(first, rem0[b] + later0, pre1[b] + early1))
        query_sum.append(jnp.where(first, suf1[b] + later1, loc0[b] + early0))
    rows_ref[...] = jnp.concatenate(loc0 + suf1 + rem0 + pre1 + tile0 + tile1, axis=0)
    tiles = []
    for t in range(4):
        pair = slice(2 * t, 2 * t + 2)
        tiles += [jnp.exp(k) for k in key_sum[pair]]
        tiles += [jnp.exp(q) * 0.0625 for q in query_sum[pair]]
        tiles += loc0[pair] + suf1[pair]
    factors_ref[...] = jnp.concatenate(tiles, axis=0)


def upright(factors):
    turned = jnp.transpose(factors)
    pairs = [(turned[:, 2 * k : 2 * k + 1], turned[:, 2 * k + 1 : 2 * k + 2]) for k in range(4)]
    return [jnp.concatenate(pair, axis=0) for pair in pairs]


def wide(rows, base, t):
    return jnp.concatenate([rows[base + 2 * t : base + 2 * t + 1], rows[base + 2 * t + 1 : base + 2 * t + 2]], axis=1)


def boundary_kernel(units_ref, factors_ref, state_ref):
    sides = [upright(factors_ref[8 * t : 8 * t + 8, :]) for t in range(4)]
    to_end = jnp.concatenate([side[0] for side in sides], axis=0)
    from_end = jnp.concatenate([side[1] for side in sides], axis=0)
    keys = (units_ref[:, 256:512].astype(F32) * to_end).astype(BF16)
    queries = (units_ref[:, 0:256].astype(F32) * from_end).astype(BF16)
    state_ref[0] = dot(keys, units_ref[:, 512:1024], TN).astype(BF16)
    state_ref[1] = dot(queries, units_ref[:, 1024:1536], TN).astype(BF16)


def inside_kernel(units_ref, rows_ref, factors_ref, out_ref, s_ref, gs_ref):
    rows = rows_ref[...]
    row = lax.broadcasted_iota(jnp.int32, (TILE, TILE), 0)
    col = lax.broadcasted_iota(jnp.int32, (TILE, TILE), 1)
    for i in range(4):
        at = pl.ds(i * TILE, TILE)
        query, grad = units_ref[at, 0:256], units_ref[at, 1024:1536]
        loc0, suf1 = upright(factors_ref[8 * i : 8 * i + 8, :])[2:]
        for j in range(4):
            to = pl.ds(j * TILE, TILE)
            if i == j:
                spread = jnp.where(row >= col, loc0 - wide(rows, 0, i), suf1 - wide(rows, 8, i))
            elif i > j:
                along = wide(rows, 16, j)
                for t in range(j + 1, i):
                    along = along + jnp.concatenate([rows[32 + t : 33 + t]] * 2, axis=1)
                spread = loc0 + along
            else:
                along = wide(rows, 24, j)
                for t in range(i + 1, j):
                    along = along + jnp.concatenate([rows[36 + t : 37 + t]] * 2, axis=1)
                spread = suf1 + along
            weights = jnp.exp(spread) * 0.0625
            scores = dot(query, units_ref[to, 256:512], NT)
            grads = dot(grad, units_ref[to, 512:1024], NT)
            s_ref[at, to] = (scores * weights).astype(BF16)
            gs_ref[at, to] = (grads * weights).astype(BF16)
    out_ref[:, 0:256] = dot(gs_ref[...], units_ref[:, 0:256], TN).astype(BF16)
    out_ref[:, 256:512] = dot(gs_ref[...], units_ref[:, 256:512], NN).astype(BF16)
    out_ref[:, 512:1024] = dot(s_ref[...], units_ref[:, 1024:1536], TN).astype(BF16)


def across_kernel(units_ref, factors_ref, state_ref, part_ref, out_ref):
    memory, later = state_ref[0], state_ref[1]
    to_end, from_end = upright(factors_ref[...])[:2]
    keys = (units_ref[:, 256:512].astype(F32) * to_end).astype(BF16)
    part = dot(units_ref[:, 512:1024], later, NT) * to_end
    out_ref[:, 0:256] = (part_ref[:, 0:256].astype(F32) + part).astype(BF16)
    part = dot(units_ref[:, 1024:1536], memory, NT) * from_end
    out_ref[:, 256:512] = (part_ref[:, 256:512].astype(F32) + part).astype(BF16)
    part = dot(keys, later, NN)
    out_ref[:, 512:1024] = (part_ref[:, 512:1024].astype(F32) + part).astype(BF16)


def kernel(body, out_shape, flops, scratch=(), **grid):
    return pl.pallas_call(
        body,
        out_shape=out_shape,
        scratch_shapes=scratch,
        cost_estimate=pl.CostEstimate(flops=flops, bytes_accessed=4 << 20, transcendentals=0),
        compiler_params=pltpu.CompilerParams(vmem_limit_bytes=24 << 20),
        **grid,
    )


def in_hbm(array):
    return pltpu.with_memory_space_constraint(array, pltpu.HBM)


def shape(dims, dtype):
    return jax.ShapeDtypeStruct(dims, dtype)


PARTS = 4


def pack_kernel(half_ref, *refs):
    sources, (out_ref,), stages, packed_ref, in_sems, out_sems = (
        refs[:4],
        refs[4:5],
        refs[5:9],
        refs[9],
        refs[10],
        refs[11],
    )
    span = BLOCK // PARTS
    loads, stores = [], []
    for p in range(PARTS):
        rows = pl.ds(p * span, span)
        for k, (source, stage) in enumerate(zip(sources, stages, strict=True)):
            loads.append(
                pltpu.make_async_copy(source.at[rows, :], stage.at[rows, :], in_sems.at[p * 4 + k])
            )
        stores.append(
            pltpu.make_async_copy(packed_ref.at[p], out_ref.at[:, rows, :], out_sems.at[p])
        )
    for load in loads:
        load.start()
    for p in range(PARTS):
        rows = pl.ds(p * span, span)
        for load in loads[4 * p : 4 * p + 4]:
            load.wait()
        for h in range(HEADS):
            lane, at = (h + 4 * half_ref[0]) & 7, 0
            for stage in stages:
                width = stage.shape[1] // HEADS
                packed_ref[p, lane, :, at : at + width] = stage[rows, h * width : h * width + width]
                at += width
        stores[p].start()
    for store in stores:
        store.wait()


def pack(half, arrays):
    outside = pl.BlockSpec(memory_space=pltpu.HBM)
    return pl.pallas_call(
        pack_kernel,
        out_shape=pltpu.HBM((HEADS, BLOCK, 1536), BF16),
        in_specs=[pl.BlockSpec(memory_space=pltpu.SMEM)] + [outside] * 4,
        out_specs=outside,
        scratch_shapes=[
            *[pltpu.VMEM(a.shape, BF16) for a in arrays],
            pltpu.VMEM((PARTS, HEADS, BLOCK // PARTS, 1536), BF16),
            pltpu.SemaphoreType.DMA((4 * PARTS,)),
            pltpu.SemaphoreType.DMA((PARTS,)),
        ],
        cost_estimate=pl.CostEstimate(flops=1 << 20, bytes_accessed=6 << 20, transcendentals=0),
        compiler_params=pltpu.CompilerParams(vmem_limit_bytes=16 << 20),
    )(half.reshape(1), *[in_hbm(a) for a in arrays])


def worker(half, head):
    return half * 8 + (head + 4 * half) % 8


STEPS = ((0, 0), (1, 0), (0, 3), (0, 1), (1, 3), (1, 1), (0, 2), (1, 2))


def term_kernel(place_ref, grads_ref, *refs):
    pieces, (mine_ref, *theirs), total_ref = refs[:8], refs[8:-1], refs[-1]
    lane = place_ref[0]
    deep, y = lane // 4, lane % 4
    total = None
    for piece, (other, step) in zip(pieces, STEPS, strict=True):
        block = (deep ^ other) * 4 + (y + step) % 4
        grad = grads_ref[pl.ds(pl.multiple_of(block * BLOCK, BLOCK), BLOCK), :]
        part = dot(piece[0], grad, TN)
        total = part if total is None else total + part
    slices = mine_ref.shape[0] * (1 + len(theirs))
    total_ref[...] = total.reshape(slices, -1, total.shape[1])
    for k in range(mine_ref.shape[0]):
        if theirs:
            mine_ref[k] = total_ref[2 * k + place_ref[1]]
            theirs[0][k] = total_ref[2 * k + 1 - place_ref[1]].astype(BF16)
        else:
            mine_ref[k] = total_ref[k]


def core_sum_kernel(turn_ref, mine_ref, theirs_ref, own_ref, *send_refs):
    ring = mine_ref.shape[0]
    for step, ref in enumerate((own_ref, *send_refs)):
        at = (turn_ref[0] + step) & (ring - 1)
        ref[...] = (mine_ref[at] + theirs_ref[at].astype(F32)).astype(ref.dtype)


def ring_sum_kernel(*refs):
    total = refs[0][...]
    for ref in refs[1:-2]:
        total = total + ref[...].astype(F32)
    refs[-2][...] = total
    refs[-1][...] = total.astype(BF16)


def half_sum_kernel(mine_ref, theirs_ref, out_ref):
    total = (mine_ref[...] + theirs_ref[...].astype(F32)).astype(BF16)
    for k in range(out_ref.shape[0]):
        out_ref[k] = total


def home_kernel(half_ref, owner_ref, home_ref, *refs):
    weights, (query_ref, value_ref, input_ref, key_ref) = refs[:-4], refs[-4:]
    for h in range(HEADS):
        lane = (h + 4 * half_ref[0]) & 7
        key_ref[:, h * 256 : h * 256 + 256] = home_ref[lane, :, 0:256]
        query_ref[:, h * 256 : h * 256 + 256] = home_ref[lane, :, 256:512]
        value_ref[:, h * 512 : h * 512 + 512] = home_ref[lane, :, 512:1024]
    for k, weight in enumerate(weights):
        span = weight.shape[0]
        at = pl.multiple_of(owner_ref[k] * span, span)
        input_ref[:, pl.ds(at, span)] = dot(key_ref[...], weight[...], NT).astype(BF16)


def widen_kernel(half_ref, in_ref, out_ref):
    for k in range(HEADS):
        at = pl.multiple_of(((k + 4 * half_ref[0]) & 7) * 256, 256)
        out_ref[:, pl.ds(at, 256)] = in_ref[k].astype(F32)


def shards(layer_input, queries, key_vectors, values, cotangent, log_decay, key_weight):
    tokens = layer_input.shape[1]
    half = lax.axis_index("half")
    lane = lax.axis_index("lane")
    peers = lax.axis_size(SP)
    ring = lax.axis_size("dp_0")
    cores = lax.axis_size("dp_1")
    core, turn = lax.axis_index("dp_1"), lax.axis_index("dp_0")

    decay = log_decay.reshape(2, 8, BLOCK)
    own = lane % 2
    near = lax.dynamic_index_in_dim(decay, own, 0, keepdims=False)
    far = lax.dynamic_index_in_dim(decay, 1 - own, 0, keepdims=False)
    near = lax.ppermute(near, SP, [(u, worker(u % 2, u // 2)) for u in range(peers)])
    far = lax.ppermute(far, SP, [(u, worker(1 - u % 2, u // 2)) for u in range(peers)])
    deep = lax.ppermute(layer_input, "lane", [(i, (i + 4) % 8) for i in range(8)])
    lam = jnp.where(half == 0, jnp.concatenate([near, far]), jnp.concatenate([far, near]))
    rows, factors = kernel(decay_kernel, (shape((40, 128), F32), shape((32, 128), F32)), 1 << 20)(
        lam, jnp.full((1, 128), half, jnp.int32)
    )

    whole = pl.BlockSpec(memory_space=pltpu.VMEM)
    scalars = pl.BlockSpec(memory_space=pltpu.SMEM)
    sent = pack(half, [a[0] for a in (queries, key_vectors, values, cotangent)])
    units = lax.all_to_all(sent, "lane", 0, 0, tiled=True).reshape(8 * tokens, -1)

    def lane_step(array, step):
        return lax.ppermute(
            array, "lane", [(i, i // 4 * 4 + (i + step) % 4) for i in range(8)]
        )

    weights, owners = [key_weight], [turn * cores + core]
    for step in range(1, ring):
        moves = [(i, (i + step) % ring) for i in range(ring)]
        weights.append(lax.ppermute(key_weight, "dp_0", moves))
        owners.append((turn - step) % ring * cores + core)
    if cores == 2:
        weights += [lax.ppermute(w, "dp_1", [(0, 1), (1, 0)]) for w in weights]
        owners += [o + 1 - 2 * core for o in owners]

    own = layer_input
    own_last = lane_step(own, 2)
    own_before, own_after = lane_step(own, 1), lane_step(own, 3)
    deep_before, deep_after = lane_step(deep, 1), lane_step(deep, 3)
    deep_last = lax.ppermute(own_last, "lane", [(i, (i + 4) % 8) for i in range(8)])

    state = kernel(boundary_kernel, pltpu.HBM((2, 256, 512), BF16), 540 << 20)(units, factors)
    state = lax.ppermute(state, SP, [(u, u ^ 12) for u in range(peers)])
    part = kernel(
        inside_kernel,
        pltpu.HBM((1024, 1024), BF16),
        3760 << 20,
        (pltpu.VMEM((1024, 1024), BF16), pltpu.VMEM((1024, 1024), BF16)),
    )(units, rows, factors)

    def by_tile(width):
        return pl.BlockSpec((TILE, width), lambda i: (i, 0))

    grads = kernel(
        across_kernel,
        pltpu.HBM((1024, 1024), BF16),
        800 << 20,
        grid=(4,),
        in_specs=[
            by_tile(1536),
            pl.BlockSpec((8, 128), lambda i: (i, 0)),
            pl.BlockSpec((2, 256, 512), lambda i: (0, 0, 0)),
            by_tile(1024),
        ],
        out_specs=by_tile(1024),
    )(units, factors, state, in_hbm(part))

    home = lax.all_to_all(grads.reshape(8, tokens, -1), "lane", 0, 0, tiled=True)
    grad_query, grad_value, grad_input = kernel(
        home_kernel,
        (shape((tokens, 2048), BF16), shape((tokens, 4096), BF16), shape((tokens, 2048), BF16)),
        1070 << 20,
        (pltpu.VMEM((tokens, 2048), BF16),),
        in_specs=[scalars] * 2 + [whole] * (1 + len(weights)),
        out_specs=(whole, whole, whole),
    )(half.reshape(1), jnp.stack(owners), home, *weights)

    parts = [shape((ring, 2048 // ring // cores, 256), F32)]
    if cores == 2:
        parts.append(pltpu.HBM((ring, 2048 // ring // cores, 256), BF16))
    terms, *theirs = kernel(
        term_kernel,
        parts,
        1070 << 20,
        (pltpu.VMEM((ring * cores, 2048 // ring // cores, 256), F32),),
        grid=(1,),
        in_specs=[scalars, pl.BlockSpec((1024, 256), lambda i: (0, 0))] + [whole] * 8,
        out_specs=[whole] * len(parts),
    )(
        jnp.stack([lane, core]),
        in_hbm(grads),
        own,
        deep,
        own_before,
        own_after,
        deep_before,
        deep_after,
        own_last,
        deep_last,
    )

    piece = terms.shape[1:]
    sends = []
    if cores == 2:
        theirs = lax.ppermute(theirs[0], "dp_1", [(0, 1), (1, 0)])
        terms, *sends = kernel(
            core_sum_kernel,
            [shape(piece, F32)] + [shape(piece, BF16)] * (ring - 1),
            1 << 20,
            in_specs=[scalars] + [whole] * 2,
            out_specs=[whole] * ring,
        )(turn.reshape(1), terms, theirs)
        for step in range(1, ring):
            moves = [(i, (i + step) % ring) for i in range(ring)]
            sends[step - 1] = lax.ppermute(sends[step - 1], "dp_0", moves)
    mine, theirs = kernel(ring_sum_kernel, (shape(piece, F32), shape(piece, BF16)), 1 << 20)(
        terms.reshape(piece), *sends
    )
    theirs = lax.ppermute(theirs, SP, [(u, u ^ 12) for u in range(peers)])
    spread = kernel(half_sum_kernel, pltpu.HBM((8, *piece), BF16), 1 << 20)(mine, theirs)
    spread = lax.all_to_all(spread, "lane", 0, 0, tiled=True)
    grad_weight = kernel(
        widen_kernel,
        pltpu.HBM((piece[0], 2048), F32),
        1 << 20,
        in_specs=[scalars, whole],
        out_specs=whole,
    )(half.reshape(1), spread)
    return grad_query[None], grad_value[None], grad_input[None], grad_weight


def solution(mesh):
    dp = mesh.shape["dp"]
    outer = (dp // 2, 2) if dp > 1 else (1, 1)
    finer = Mesh(mesh.devices.reshape(2, 8, *outer), SP + DP)
    part = P(DP, SP, None)
    return jax.shard_map(
        shards,
        mesh=finer,
        in_specs=(part, part, part, part, part, part, P(DP, None)),
        out_specs=(part, part, part, P(DP, None)),
        check_vma=False,
    )
```

```python
import jax
import jax.numpy as jnp
from jax import lax
from jax.experimental import pallas as pl
from jax.experimental.pallas import tpu as pltpu
from jax.sharding import Mesh
from jax.sharding import PartitionSpec as P


HEADS = 8
BLOCK = 128
TILE = 256
SP = ("half", "lane")
DP = ("dp_0", "dp_1")
F32 = jnp.float32
BF16 = jnp.bfloat16


def dot(a, b, dims, precision=None):
    return lax.dot_general(a, b, (dims, ((), ())), precision=precision, preferred_element_type=F32)


NN = ((1,), (0,))
NT = ((1,), (1,))
TN = ((0,), (0,))


def decay_kernel(lam_ref, half_ref, rows_ref, factors_ref):
    n = BLOCK
    row = lax.broadcasted_iota(jnp.int32, (n, n), 0)
    col = lax.broadcasted_iota(jnp.int32, (n, n), 1)
    lam = lam_ref[...]
    high = lax.Precision.HIGHEST
    upto = dot(lam, (row <= col).astype(F32), NN, high)
    before = dot(lam, (row < col).astype(F32), NN, high)
    since = dot(lam, (row >= col).astype(F32), NN, high)
    after = dot(lam, (row > col).astype(F32), NN, high)
    totals = [jnp.broadcast_to(upto[b : b + 1, n - 1 : n], (1, n)) for b in range(16)]
    loc0, suf1, rem0, pre1 = [], [], [], []
    for b in range(8):
        odd = b % 2 == 1
        loc0.append(upto[b : b + 1] + totals[b - 1] if odd else upto[b : b + 1])
        suf1.append(since[8 + b : 9 + b] if odd else since[8 + b : 9 + b] + totals[9 + b])
        rem0.append(after[b : b + 1] if odd else after[b : b + 1] + totals[b + 1])
        pre1.append(before[8 + b : 9 + b] + totals[7 + b] if odd else before[8 + b : 9 + b])
    tile0 = [totals[2 * t] + totals[2 * t + 1] for t in range(4)]
    tile1 = [totals[8 + 2 * t] + totals[9 + 2 * t] for t in range(4)]
    first = half_ref[...] == 0
    key_sum, query_sum = [], []
    for b in range(8):
        t = b // 2
        later0, later1 = sum(tile0[t + 1 :]), sum(tile1[t + 1 :])
        early0, early1 = sum(tile0[:t]), sum(tile1[:t])
        key_sum.append(jnp.where(first, rem0[b] + later0, pre1[b] + early1))
        query_sum.append(jnp.where(first, suf1[b] + later1, loc0[b] + early0))
    rows_ref[...] = jnp.concatenate(loc0 + suf1 + rem0 + pre1 + tile0 + tile1, axis=0)
    tiles = []
    for t in range(4):
        pair = slice(2 * t, 2 * t + 2)
        tiles += [jnp.exp(k) for k in key_sum[pair]]
        tiles += [jnp.exp(q) * 0.0625 for q in query_sum[pair]]
        tiles += loc0[pair] + suf1[pair]
    factors_ref[...] = jnp.concatenate(tiles, axis=0)


def upright(factors):
    turned = jnp.transpose(factors)
    pairs = [(turned[:, 2 * k : 2 * k + 1], turned[:, 2 * k + 1 : 2 * k + 2]) for k in range(4)]
    return [jnp.concatenate(pair, axis=0) for pair in pairs]


def wide(rows, base, t):
    return jnp.concatenate([rows[base + 2 * t : base + 2 * t + 1], rows[base + 2 * t + 1 : base + 2 * t + 2]], axis=1)


def boundary_kernel(units_ref, factors_ref, state_ref):
    sides = [upright(factors_ref[8 * t : 8 * t + 8, :]) for t in range(4)]
    to_end = jnp.concatenate([side[0] for side in sides], axis=0)
    from_end = jnp.concatenate([side[1] for side in sides], axis=0)
    keys = (units_ref[:, 256:512].astype(F32) * to_end).astype(BF16)
    queries = (units_ref[:, 0:256].astype(F32) * from_end).astype(BF16)
    state_ref[0] = dot(keys, units_ref[:, 512:1024], TN).astype(BF16)
    state_ref[1] = dot(queries, units_ref[:, 1024:1536], TN).astype(BF16)


def inside_kernel(units_ref, rows_ref, factors_ref, out_ref, s_ref, gs_ref):
    rows = rows_ref[...]
    row = lax.broadcasted_iota(jnp.int32, (TILE, TILE), 0)
    col = lax.broadcasted_iota(jnp.int32, (TILE, TILE), 1)
    for i in range(4):
        at = pl.ds(i * TILE, TILE)
        query, grad = units_ref[at, 0:256], units_ref[at, 1024:1536]
        loc0, suf1 = upright(factors_ref[8 * i : 8 * i + 8, :])[2:]
        for j in range(4):
            to = pl.ds(j * TILE, TILE)
            if i == j:
                spread = jnp.where(row >= col, loc0 - wide(rows, 0, i), suf1 - wide(rows, 8, i))
            elif i > j:
                along = wide(rows, 16, j)
                for t in range(j + 1, i):
                    along = along + jnp.concatenate([rows[32 + t : 33 + t]] * 2, axis=1)
                spread = loc0 + along
            else:
                along = wide(rows, 24, j)
                for t in range(i + 1, j):
                    along = along + jnp.concatenate([rows[36 + t : 37 + t]] * 2, axis=1)
                spread = suf1 + along
            weights = jnp.exp(spread) * 0.0625
            scores = dot(query, units_ref[to, 256:512], NT)
            grads = dot(grad, units_ref[to, 512:1024], NT)
            s_ref[at, to] = (scores * weights).astype(BF16)
            gs_ref[at, to] = (grads * weights).astype(BF16)
    out_ref[:, 0:256] = dot(gs_ref[...], units_ref[:, 0:256], TN).astype(BF16)
    out_ref[:, 256:512] = dot(gs_ref[...], units_ref[:, 256:512], NN).astype(BF16)
    out_ref[:, 512:1024] = dot(s_ref[...], units_ref[:, 1024:1536], TN).astype(BF16)


def across_kernel(units_ref, factors_ref, state_ref, part_ref, out_ref):
    memory, later = state_ref[0], state_ref[1]
    to_end, from_end = upright(factors_ref[...])[:2]
    keys = (units_ref[:, 256:512].astype(F32) * to_end).astype(BF16)
    part = dot(units_ref[:, 512:1024], later, NT) * to_end
    out_ref[:, 0:256] = (part_ref[:, 0:256].astype(F32) + part).astype(BF16)
    part = dot(units_ref[:, 1024:1536], memory, NT) * from_end
    out_ref[:, 256:512] = (part_ref[:, 256:512].astype(F32) + part).astype(BF16)
    part = dot(keys, later, NN)
    out_ref[:, 512:1024] = (part_ref[:, 512:1024].astype(F32) + part).astype(BF16)


def kernel(body, out_shape, flops, scratch=(), **grid):
    return pl.pallas_call(
        body,
        out_shape=out_shape,
        scratch_shapes=scratch,
        cost_estimate=pl.CostEstimate(flops=flops, bytes_accessed=4 << 20, transcendentals=0),
        compiler_params=pltpu.CompilerParams(vmem_limit_bytes=24 << 20),
        **grid,
    )


def in_hbm(array):
    return pltpu.with_memory_space_constraint(array, pltpu.HBM)


def shape(dims, dtype):
    return jax.ShapeDtypeStruct(dims, dtype)


PARTS = 4


def pack_kernel(half_ref, *refs):
    sources, (out_ref,), stages, packed_ref, in_sems, out_sems = (
        refs[:4],
        refs[4:5],
        refs[5:9],
        refs[9],
        refs[10],
        refs[11],
    )
    span = BLOCK // PARTS
    loads, stores = [], []
    for p in range(PARTS):
        rows = pl.ds(p * span, span)
        for k, (source, stage) in enumerate(zip(sources, stages, strict=True)):
            loads.append(
                pltpu.make_async_copy(source.at[rows, :], stage.at[rows, :], in_sems.at[p * 4 + k])
            )
        stores.append(
            pltpu.make_async_copy(packed_ref.at[p], out_ref.at[:, rows, :], out_sems.at[p])
        )
    for load in loads:
        load.start()
    for p in range(PARTS):
        rows = pl.ds(p * span, span)
        for load in loads[4 * p : 4 * p + 4]:
            load.wait()
        for h in range(HEADS):
            lane, at = (h + 4 * half_ref[0]) & 7, 0
            for stage in stages:
                width = stage.shape[1] // HEADS
                packed_ref[p, lane, :, at : at + width] = stage[rows, h * width : h * width + width]
                at += width
        stores[p].start()
    for store in stores:
        store.wait()


def pack(half, arrays):
    outside = pl.BlockSpec(memory_space=pltpu.HBM)
    return pl.pallas_call(
        pack_kernel,
        out_shape=pltpu.HBM((HEADS, BLOCK, 1536), BF16),
        in_specs=[pl.BlockSpec(memory_space=pltpu.SMEM)] + [outside] * 4,
        out_specs=outside,
        scratch_shapes=[
            *[pltpu.VMEM(a.shape, BF16) for a in arrays],
            pltpu.VMEM((PARTS, HEADS, BLOCK // PARTS, 1536), BF16),
            pltpu.SemaphoreType.DMA((4 * PARTS,)),
            pltpu.SemaphoreType.DMA((PARTS,)),
        ],
        cost_estimate=pl.CostEstimate(flops=1 << 20, bytes_accessed=6 << 20, transcendentals=0),
        compiler_params=pltpu.CompilerParams(vmem_limit_bytes=16 << 20),
    )(half.reshape(1), *[in_hbm(a) for a in arrays])


def worker(half, head):
    return half * 8 + (head + 4 * half) % 8


EARLY = ((0, 0), (1, 0), (0, 3), (0, 1), (0, 2))
LATE = ((1, 2), (1, 3), (1, 1))


def term_sum(lane, grads_ref, pieces, steps, total):
    deep, y = lane // 4, lane % 4
    for piece, (other, step) in zip(pieces, steps, strict=True):
        block = (deep ^ other) * 4 + (y + step) % 4
        grad = grads_ref[pl.ds(pl.multiple_of(block * BLOCK, BLOCK), BLOCK), :]
        part = dot(piece[0], grad, TN)
        total = part if total is None else total + part
    return total


def early_kernel(place_ref, grads_ref, *refs):
    refs[-1][...] = term_sum(place_ref[0], grads_ref, refs[:-1], EARLY, None)


def late_kernel(place_ref, grads_ref, early_ref, *refs):
    pieces, (mine_ref, *theirs), total_ref = refs[: len(LATE)], refs[len(LATE) : -1], refs[-1]
    total = term_sum(place_ref[0], grads_ref, pieces, LATE, early_ref[...])
    slices = mine_ref.shape[0] * (1 + len(theirs))
    total_ref[...] = total.reshape(slices, -1, total.shape[1])
    for k in range(mine_ref.shape[0]):
        if theirs:
            mine_ref[k] = total_ref[2 * k + place_ref[1]]
            theirs[0][k] = total_ref[2 * k + 1 - place_ref[1]].astype(BF16)
        else:
            mine_ref[k] = total_ref[k]


def core_sum_kernel(turn_ref, mine_ref, theirs_ref, own_ref, *send_refs):
    ring = mine_ref.shape[0]
    for step, ref in enumerate((own_ref, *send_refs)):
        at = (turn_ref[0] + step) & (ring - 1)
        ref[...] = (mine_ref[at] + theirs_ref[at].astype(F32)).astype(ref.dtype)


def ring_sum_kernel(*refs):
    total = refs[0][...]
    for ref in refs[1:-2]:
        total = total + ref[...].astype(F32)
    refs[-2][...] = total
    refs[-1][...] = total.astype(BF16)


def half_sum_kernel(mine_ref, theirs_ref, out_ref):
    total = (mine_ref[...] + theirs_ref[...].astype(F32)).astype(BF16)
    for k in range(out_ref.shape[0]):
        out_ref[k] = total


def home_kernel(half_ref, owner_ref, home_ref, *refs):
    weights, (query_ref, value_ref, input_ref, key_ref) = refs[:-4], refs[-4:]
    for h in range(HEADS):
        lane = (h + 4 * half_ref[0]) & 7
        key_ref[:, h * 256 : h * 256 + 256] = home_ref[lane, :, 0:256]
        query_ref[:, h * 256 : h * 256 + 256] = home_ref[lane, :, 256:512]
        value_ref[:, h * 512 : h * 512 + 512] = home_ref[lane, :, 512:1024]
    for k, weight in enumerate(weights):
        span = weight.shape[0]
        at = pl.multiple_of(owner_ref[k] * span, span)
        input_ref[:, pl.ds(at, span)] = dot(key_ref[...], weight[...], NT).astype(BF16)


def widen_kernel(half_ref, in_ref, out_ref):
    for k in range(HEADS):
        at = pl.multiple_of(((k + 4 * half_ref[0]) & 7) * 256, 256)
        out_ref[:, pl.ds(at, 256)] = in_ref[k].astype(F32)


def shards(layer_input, queries, key_vectors, values, cotangent, log_decay, key_weight):
    tokens = layer_input.shape[1]
    half = lax.axis_index("half")
    lane = lax.axis_index("lane")
    peers = lax.axis_size(SP)
    ring = lax.axis_size("dp_0")
    cores = lax.axis_size("dp_1")
    core, turn = lax.axis_index("dp_1"), lax.axis_index("dp_0")

    decay = log_decay.reshape(2, 8, BLOCK)
    own = lane % 2
    near = lax.dynamic_index_in_dim(decay, own, 0, keepdims=False)
    far = lax.dynamic_index_in_dim(decay, 1 - own, 0, keepdims=False)
    near = lax.ppermute(near, SP, [(u, worker(u % 2, u // 2)) for u in range(peers)])
    far = lax.ppermute(far, SP, [(u, worker(1 - u % 2, u // 2)) for u in range(peers)])
    deep = lax.ppermute(layer_input, "lane", [(i, (i + 4) % 8) for i in range(8)])
    lam = jnp.where(half == 0, jnp.concatenate([near, far]), jnp.concatenate([far, near]))
    rows, factors = kernel(decay_kernel, (shape((40, 128), F32), shape((32, 128), F32)), 1 << 20)(
        lam, jnp.full((1, 128), half, jnp.int32)
    )

    whole = pl.BlockSpec(memory_space=pltpu.VMEM)
    scalars = pl.BlockSpec(memory_space=pltpu.SMEM)
    sent = pack(half, [a[0] for a in (queries, key_vectors, values, cotangent)])
    units = lax.all_to_all(sent, "lane", 0, 0, tiled=True).reshape(8 * tokens, -1)

    def lane_step(array, step):
        return lax.ppermute(
            array, "lane", [(i, i // 4 * 4 + (i + step) % 4) for i in range(8)]
        )

    weights, owners = [key_weight], [turn * cores + core]
    for step in range(1, ring):
        moves = [(i, (i + step) % ring) for i in range(ring)]
        weights.append(lax.ppermute(key_weight, "dp_0", moves))
        owners.append((turn - step) % ring * cores + core)
    if cores == 2:
        weights += [lax.ppermute(w, "dp_1", [(0, 1), (1, 0)]) for w in weights]
        owners += [o + 1 - 2 * core for o in owners]

    own = layer_input
    own_last = lane_step(own, 2)
    own_before, own_after = lane_step(own, 1), lane_step(own, 3)
    deep_before, deep_after = lane_step(deep, 1), lane_step(deep, 3)
    deep_last = lax.ppermute(own_last, "lane", [(i, (i + 4) % 8) for i in range(8)])

    state = kernel(boundary_kernel, pltpu.HBM((2, 256, 512), BF16), 540 << 20)(units, factors)
    state = lax.ppermute(state, SP, [(u, u ^ 12) for u in range(peers)])
    part = kernel(
        inside_kernel,
        pltpu.HBM((1024, 1024), BF16),
        3760 << 20,
        (pltpu.VMEM((1024, 1024), BF16), pltpu.VMEM((1024, 1024), BF16)),
    )(units, rows, factors)

    def by_tile(width):
        return pl.BlockSpec((TILE, width), lambda i: (i, 0))

    grads = kernel(
        across_kernel,
        pltpu.HBM((1024, 1024), BF16),
        800 << 20,
        grid=(4,),
        in_specs=[
            by_tile(1536),
            pl.BlockSpec((8, 128), lambda i: (i, 0)),
            pl.BlockSpec((2, 256, 512), lambda i: (0, 0, 0)),
            by_tile(1024),
        ],
        out_specs=by_tile(1024),
    )(units, factors, state, in_hbm(part))

    home = lax.all_to_all(grads.reshape(8, tokens, -1), "lane", 0, 0, tiled=True)
    grad_query, grad_value, grad_input = kernel(
        home_kernel,
        (shape((tokens, 2048), BF16), shape((tokens, 4096), BF16), shape((tokens, 2048), BF16)),
        1070 << 20,
        (pltpu.VMEM((tokens, 2048), BF16),),
        in_specs=[scalars] * 2 + [whole] * (1 + len(weights)),
        out_specs=(whole, whole, whole),
    )(half.reshape(1), jnp.stack(owners), home, *weights)

    parts = [shape((ring, 2048 // ring // cores, 256), F32)]
    if cores == 2:
        parts.append(pltpu.HBM((ring, 2048 // ring // cores, 256), BF16))
    place = jnp.stack([lane, core])
    first = pl.BlockSpec((1024, 256), lambda i: (0, 0))
    early = kernel(
        early_kernel,
        shape((2048, 256), F32),
        670 << 20,
        grid=(1,),
        in_specs=[scalars, first] + [whole] * len(EARLY),
        out_specs=whole,
    )(place, in_hbm(grads), own, deep, own_before, own_after, own_last)
    terms, *theirs = kernel(
        late_kernel,
        parts,
        400 << 20,
        (pltpu.VMEM((ring * cores, 2048 // ring // cores, 256), F32),),
        grid=(1,),
        in_specs=[scalars, first] + [whole] * (1 + len(LATE)),
        out_specs=[whole] * len(parts),
    )(place, in_hbm(grads), early, deep_last, deep_before, deep_after)

    piece = terms.shape[1:]
    sends = []
    if cores == 2:
        theirs = lax.ppermute(theirs[0], "dp_1", [(0, 1), (1, 0)])
        terms, *sends = kernel(
            core_sum_kernel,
            [shape(piece, F32)] + [shape(piece, BF16)] * (ring - 1),
            1 << 20,
            in_specs=[scalars] + [whole] * 2,
            out_specs=[whole] * ring,
        )(turn.reshape(1), terms, theirs)
        for step in range(1, ring):
            moves = [(i, (i + step) % ring) for i in range(ring)]
            sends[step - 1] = lax.ppermute(sends[step - 1], "dp_0", moves)
    mine, theirs = kernel(ring_sum_kernel, (shape(piece, F32), shape(piece, BF16)), 1 << 20)(
        terms.reshape(piece), *sends
    )
    theirs = lax.ppermute(theirs, SP, [(u, u ^ 12) for u in range(peers)])
    spread = kernel(half_sum_kernel, pltpu.HBM((8, *piece), BF16), 1 << 20)(mine, theirs)
    spread = lax.all_to_all(spread, "lane", 0, 0, tiled=True)
    grad_weight = kernel(
        widen_kernel,
        pltpu.HBM((piece[0], 2048), F32),
        1 << 20,
        in_specs=[scalars, whole],
        out_specs=whole,
    )(half.reshape(1), spread)
    return grad_query[None], grad_value[None], grad_input[None], grad_weight


def solution(mesh):
    dp = mesh.shape["dp"]
    outer = (dp // 2, 2) if dp > 1 else (1, 1)
    finer = Mesh(mesh.devices.reshape(2, 8, *outer), SP + DP)
    part = P(DP, SP, None)
    return jax.shard_map(
        shards,
        mesh=finer,
        in_specs=(part, part, part, part, part, part, P(DP, None)),
        out_specs=(part, part, part, P(DP, None)),
        check_vma=False,
    )
```

```python
import functools

import jax
import jax.numpy as jnp
from jax import lax
from jax.experimental import pallas as pl
from jax.experimental.pallas import tpu as pltpu
from jax.sharding import Mesh
from jax.sharding import PartitionSpec as P


HEADS = 8
BLOCK = 128
TILE = 256
SP = ("half", "lane")
DP = ("dp_0", "dp_1")
F32 = jnp.float32
BF16 = jnp.bfloat16


def dot(a, b, dims, precision=None):
    return lax.dot_general(a, b, (dims, ((), ())), precision=precision, preferred_element_type=F32)


NN = ((1,), (0,))
NT = ((1,), (1,))
TN = ((0,), (0,))


def decay_kernel(lam_ref, half_ref, rows_ref, factors_ref):
    n = BLOCK
    row = lax.broadcasted_iota(jnp.int32, (n, n), 0)
    col = lax.broadcasted_iota(jnp.int32, (n, n), 1)
    lam = lam_ref[...]
    high = lax.Precision.HIGHEST
    upto = dot(lam, (row <= col).astype(F32), NN, high)
    before = dot(lam, (row < col).astype(F32), NN, high)
    since = dot(lam, (row >= col).astype(F32), NN, high)
    after = dot(lam, (row > col).astype(F32), NN, high)
    totals = [jnp.broadcast_to(upto[b : b + 1, n - 1 : n], (1, n)) for b in range(16)]
    loc0, suf1, rem0, pre1 = [], [], [], []
    for b in range(8):
        odd = b % 2 == 1
        loc0.append(upto[b : b + 1] + totals[b - 1] if odd else upto[b : b + 1])
        suf1.append(since[8 + b : 9 + b] if odd else since[8 + b : 9 + b] + totals[9 + b])
        rem0.append(after[b : b + 1] if odd else after[b : b + 1] + totals[b + 1])
        pre1.append(before[8 + b : 9 + b] + totals[7 + b] if odd else before[8 + b : 9 + b])
    tile0 = [totals[2 * t] + totals[2 * t + 1] for t in range(4)]
    tile1 = [totals[8 + 2 * t] + totals[9 + 2 * t] for t in range(4)]
    first = half_ref[...] == 0
    key_sum, query_sum = [], []
    for b in range(8):
        t = b // 2
        later0, later1 = sum(tile0[t + 1 :]), sum(tile1[t + 1 :])
        early0, early1 = sum(tile0[:t]), sum(tile1[:t])
        key_sum.append(jnp.where(first, rem0[b] + later0, pre1[b] + early1))
        query_sum.append(jnp.where(first, suf1[b] + later1, loc0[b] + early0))
    rows_ref[...] = jnp.concatenate(loc0 + suf1 + rem0 + pre1 + tile0 + tile1, axis=0)
    tiles = []
    for t in range(4):
        pair = slice(2 * t, 2 * t + 2)
        tiles += [jnp.exp(k) for k in key_sum[pair]]
        tiles += [jnp.exp(q) * 0.0625 for q in query_sum[pair]]
        tiles += loc0[pair] + suf1[pair]
    factors_ref[...] = jnp.concatenate(tiles, axis=0)


def upright(factors):
    turned = jnp.transpose(factors)
    pairs = [(turned[:, 2 * k : 2 * k + 1], turned[:, 2 * k + 1 : 2 * k + 2]) for k in range(4)]
    return [jnp.concatenate(pair, axis=0) for pair in pairs]


def wide(rows, base, t):
    return jnp.concatenate([rows[base + 2 * t : base + 2 * t + 1], rows[base + 2 * t + 1 : base + 2 * t + 2]], axis=1)


def boundary_kernel(units_ref, factors_ref, state_ref):
    sides = [upright(factors_ref[8 * t : 8 * t + 8, :]) for t in range(4)]
    to_end = jnp.concatenate([side[0] for side in sides], axis=0)
    from_end = jnp.concatenate([side[1] for side in sides], axis=0)
    keys = (units_ref[:, 256:512].astype(F32) * to_end).astype(BF16)
    queries = (units_ref[:, 0:256].astype(F32) * from_end).astype(BF16)
    state_ref[0] = dot(keys, units_ref[:, 512:1024], TN).astype(BF16)
    state_ref[1] = dot(queries, units_ref[:, 1024:1536], TN).astype(BF16)


def inside_kernel(units_ref, rows_ref, factors_ref, out_ref, s_ref, gs_ref):
    rows = rows_ref[...]
    row = lax.broadcasted_iota(jnp.int32, (TILE, TILE), 0)
    col = lax.broadcasted_iota(jnp.int32, (TILE, TILE), 1)
    for i in range(4):
        at = pl.ds(i * TILE, TILE)
        query, grad = units_ref[at, 0:256], units_ref[at, 1024:1536]
        loc0, suf1 = upright(factors_ref[8 * i : 8 * i + 8, :])[2:]
        for j in range(4):
            to = pl.ds(j * TILE, TILE)
            if i == j:
                spread = jnp.where(row >= col, loc0 - wide(rows, 0, i), suf1 - wide(rows, 8, i))
            elif i > j:
                along = wide(rows, 16, j)
                for t in range(j + 1, i):
                    along = along + jnp.concatenate([rows[32 + t : 33 + t]] * 2, axis=1)
                spread = loc0 + along
            else:
                along = wide(rows, 24, j)
                for t in range(i + 1, j):
                    along = along + jnp.concatenate([rows[36 + t : 37 + t]] * 2, axis=1)
                spread = suf1 + along
            weights = jnp.exp(spread) * 0.0625
            scores = dot(query, units_ref[to, 256:512], NT)
            grads = dot(grad, units_ref[to, 512:1024], NT)
            s_ref[at, to] = (scores * weights).astype(BF16)
            gs_ref[at, to] = (grads * weights).astype(BF16)
    out_ref[:, 0:256] = dot(gs_ref[...], units_ref[:, 0:256], TN).astype(BF16)
    out_ref[:, 256:512] = dot(gs_ref[...], units_ref[:, 256:512], NN).astype(BF16)
    out_ref[:, 512:1024] = dot(s_ref[...], units_ref[:, 1024:1536], TN).astype(BF16)


def across_kernel(units_ref, factors_ref, state_ref, part_ref, out_ref):
    memory, later = state_ref[0], state_ref[1]
    to_end, from_end = upright(factors_ref[...])[:2]
    keys = (units_ref[:, 256:512].astype(F32) * to_end).astype(BF16)
    part = dot(units_ref[:, 512:1024], later, NT) * to_end
    out_ref[:, 0:256] = (part_ref[:, 0:256].astype(F32) + part).astype(BF16)
    part = dot(units_ref[:, 1024:1536], memory, NT) * from_end
    out_ref[:, 256:512] = (part_ref[:, 256:512].astype(F32) + part).astype(BF16)
    part = dot(keys, later, NN)
    out_ref[:, 512:1024] = (part_ref[:, 512:1024].astype(F32) + part).astype(BF16)


def kernel(body, out_shape, flops, scratch=(), **grid):
    return pl.pallas_call(
        body,
        out_shape=out_shape,
        scratch_shapes=scratch,
        cost_estimate=pl.CostEstimate(flops=flops, bytes_accessed=4 << 20, transcendentals=0),
        compiler_params=pltpu.CompilerParams(vmem_limit_bytes=24 << 20),
        **grid,
    )


def in_hbm(array):
    return pltpu.with_memory_space_constraint(array, pltpu.HBM)


def shape(dims, dtype):
    return jax.ShapeDtypeStruct(dims, dtype)


PARTS = 4


def pack_kernel(half_ref, *refs):
    sources, (out_ref,), stages, packed_ref, in_sems, out_sems = (
        refs[:4],
        refs[4:5],
        refs[5:9],
        refs[9],
        refs[10],
        refs[11],
    )
    span = BLOCK // PARTS
    loads, stores = [], []
    for p in range(PARTS):
        rows = pl.ds(p * span, span)
        for k, (source, stage) in enumerate(zip(sources, stages, strict=True)):
            loads.append(
                pltpu.make_async_copy(source.at[rows, :], stage.at[rows, :], in_sems.at[p * 4 + k])
            )
        stores.append(
            pltpu.make_async_copy(packed_ref.at[p], out_ref.at[:, rows, :], out_sems.at[p])
        )
    for load in loads:
        load.start()
    for p in range(PARTS):
        rows = pl.ds(p * span, span)
        for load in loads[4 * p : 4 * p + 4]:
            load.wait()
        for h in range(HEADS):
            lane, at = (h + 4 * half_ref[0]) & 7, 0
            for stage in stages:
                width = stage.shape[1] // HEADS
                packed_ref[p, lane, :, at : at + width] = stage[rows, h * width : h * width + width]
                at += width
        stores[p].start()
    for store in stores:
        store.wait()


def pack(half, arrays):
    outside = pl.BlockSpec(memory_space=pltpu.HBM)
    return pl.pallas_call(
        pack_kernel,
        out_shape=pltpu.HBM((HEADS, BLOCK, 1536), BF16),
        in_specs=[pl.BlockSpec(memory_space=pltpu.SMEM)] + [outside] * 4,
        out_specs=outside,
        scratch_shapes=[
            *[pltpu.VMEM(a.shape, BF16) for a in arrays],
            pltpu.VMEM((PARTS, HEADS, BLOCK // PARTS, 1536), BF16),
            pltpu.SemaphoreType.DMA((4 * PARTS,)),
            pltpu.SemaphoreType.DMA((PARTS,)),
        ],
        cost_estimate=pl.CostEstimate(flops=1 << 20, bytes_accessed=6 << 20, transcendentals=0),
        compiler_params=pltpu.CompilerParams(vmem_limit_bytes=16 << 20),
    )(half.reshape(1), *[in_hbm(a) for a in arrays])


def worker(half, head):
    return half * 8 + (head + 4 * half) % 8


EARLY = ((0, 0), (1, 0), (0, 3), (0, 1), (0, 2))
LATE = ((1, 2), (1, 3), (1, 1))


def term_sum(lane, grads_ref, pieces, steps, total):
    deep, y = lane // 4, lane % 4
    for piece, (other, step) in zip(pieces, steps, strict=True):
        block = (deep ^ other) * 4 + (y + step) % 4
        grad = grads_ref[pl.ds(pl.multiple_of(block * BLOCK, BLOCK), BLOCK), :]
        part = dot(piece[0], grad, TN)
        total = part if total is None else total + part
    return total


def early_kernel(place_ref, grads_ref, *refs):
    refs[-1][...] = term_sum(place_ref[0], grads_ref, refs[:-1], EARLY, None)


def late_kernel(side, place_ref, grads_ref, early_ref, *refs):
    pieces, out_ref = refs[:-1], refs[-1]
    ring, span, _ = out_ref.shape
    cores = early_ref.shape[0] // (ring * span)
    lane = place_ref[0]
    deep, y = lane // 4, lane % 4
    grads = []
    for other, step in LATE:
        block = (deep ^ other) * 4 + (y + step) % 4
        grads.append(grads_ref[pl.ds(pl.multiple_of(block * BLOCK, BLOCK), BLOCK), :])
    for k in range(ring):
        owner = cores * k + (place_ref[1] if side == 0 else 1 - place_ref[1])
        at = pl.multiple_of(owner * span, span)
        total = early_ref[pl.ds(at, span), :]
        for piece, grad in zip(pieces, grads, strict=True):
            total = total + dot(piece[0, :, pl.ds(at, span)], grad, TN)
        out_ref[k] = total.astype(out_ref.dtype)


def core_sum_kernel(turn_ref, mine_ref, theirs_ref, own_ref, *send_refs):
    ring = mine_ref.shape[0]
    for step, ref in enumerate((own_ref, *send_refs)):
        at = (turn_ref[0] + step) & (ring - 1)
        ref[...] = (mine_ref[at] + theirs_ref[at].astype(F32)).astype(ref.dtype)


def ring_sum_kernel(*refs):
    total = refs[0][...]
    for ref in refs[1:-2]:
        total = total + ref[...].astype(F32)
    refs[-2][...] = total
    refs[-1][...] = total.astype(BF16)


def half_sum_kernel(mine_ref, theirs_ref, out_ref):
    total = (mine_ref[...] + theirs_ref[...].astype(F32)).astype(BF16)
    for k in range(out_ref.shape[0]):
        out_ref[k] = total


def home_kernel(half_ref, owner_ref, home_ref, *refs):
    weights, (query_ref, value_ref, input_ref, key_ref) = refs[:-4], refs[-4:]
    for h in range(HEADS):
        lane = (h + 4 * half_ref[0]) & 7
        key_ref[:, h * 256 : h * 256 + 256] = home_ref[lane, :, 0:256]
        query_ref[:, h * 256 : h * 256 + 256] = home_ref[lane, :, 256:512]
        value_ref[:, h * 512 : h * 512 + 512] = home_ref[lane, :, 512:1024]
    for k, weight in enumerate(weights):
        span = weight.shape[0]
        at = pl.multiple_of(owner_ref[k] * span, span)
        input_ref[:, pl.ds(at, span)] = dot(key_ref[...], weight[...], NT).astype(BF16)


def widen_kernel(half_ref, in_ref, out_ref):
    for k in range(HEADS):
        at = pl.multiple_of(((k + 4 * half_ref[0]) & 7) * 256, 256)
        out_ref[:, pl.ds(at, 256)] = in_ref[k].astype(F32)


def shards(layer_input, queries, key_vectors, values, cotangent, log_decay, key_weight):
    tokens = layer_input.shape[1]
    half = lax.axis_index("half")
    lane = lax.axis_index("lane")
    peers = lax.axis_size(SP)
    ring = lax.axis_size("dp_0")
    cores = lax.axis_size("dp_1")
    core, turn = lax.axis_index("dp_1"), lax.axis_index("dp_0")

    decay = log_decay.reshape(2, 8, BLOCK)
    own = lane % 2
    near = lax.dynamic_index_in_dim(decay, own, 0, keepdims=False)
    far = lax.dynamic_index_in_dim(decay, 1 - own, 0, keepdims=False)
    near = lax.ppermute(near, SP, [(u, worker(u % 2, u // 2)) for u in range(peers)])
    far = lax.ppermute(far, SP, [(u, worker(1 - u % 2, u // 2)) for u in range(peers)])
    deep = lax.ppermute(layer_input, "lane", [(i, (i + 4) % 8) for i in range(8)])
    lam = jnp.where(half == 0, jnp.concatenate([near, far]), jnp.concatenate([far, near]))
    rows, factors = kernel(decay_kernel, (shape((40, 128), F32), shape((32, 128), F32)), 1 << 20)(
        lam, jnp.full((1, 128), half, jnp.int32)
    )

    whole = pl.BlockSpec(memory_space=pltpu.VMEM)
    scalars = pl.BlockSpec(memory_space=pltpu.SMEM)
    sent = pack(half, [a[0] for a in (queries, key_vectors, values, cotangent)])
    units = lax.all_to_all(sent, "lane", 0, 0, tiled=True).reshape(8 * tokens, -1)

    def lane_step(array, step):
        return lax.ppermute(
            array, "lane", [(i, i // 4 * 4 + (i + step) % 4) for i in range(8)]
        )

    weights, owners = [key_weight], [turn * cores + core]
    for step in range(1, ring):
        moves = [(i, (i + step) % ring) for i in range(ring)]
        weights.append(lax.ppermute(key_weight, "dp_0", moves))
        owners.append((turn - step) % ring * cores + core)
    if cores == 2:
        weights += [lax.ppermute(w, "dp_1", [(0, 1), (1, 0)]) for w in weights]
        owners += [o + 1 - 2 * core for o in owners]

    own = layer_input
    own_last = lane_step(own, 2)
    own_before, own_after = lane_step(own, 1), lane_step(own, 3)
    deep_before, deep_after = lane_step(deep, 1), lane_step(deep, 3)
    deep_last = lax.ppermute(own_last, "lane", [(i, (i + 4) % 8) for i in range(8)])

    state = kernel(boundary_kernel, pltpu.HBM((2, 256, 512), BF16), 540 << 20)(units, factors)
    state = lax.ppermute(state, SP, [(u, u ^ 12) for u in range(peers)])
    part = kernel(
        inside_kernel,
        pltpu.HBM((1024, 1024), BF16),
        3760 << 20,
        (pltpu.VMEM((1024, 1024), BF16), pltpu.VMEM((1024, 1024), BF16)),
    )(units, rows, factors)

    def by_tile(width):
        return pl.BlockSpec((TILE, width), lambda i: (i, 0))

    grads = kernel(
        across_kernel,
        pltpu.HBM((1024, 1024), BF16),
        800 << 20,
        grid=(4,),
        in_specs=[
            by_tile(1536),
            pl.BlockSpec((8, 128), lambda i: (i, 0)),
            pl.BlockSpec((2, 256, 512), lambda i: (0, 0, 0)),
            by_tile(1024),
        ],
        out_specs=by_tile(1024),
    )(units, factors, state, in_hbm(part))

    home = lax.all_to_all(grads.reshape(8, tokens, -1), "lane", 0, 0, tiled=True)
    grad_query, grad_value, grad_input = kernel(
        home_kernel,
        (shape((tokens, 2048), BF16), shape((tokens, 4096), BF16), shape((tokens, 2048), BF16)),
        1070 << 20,
        (pltpu.VMEM((tokens, 2048), BF16),),
        in_specs=[scalars] * 2 + [whole] * (1 + len(weights)),
        out_specs=(whole, whole, whole),
    )(half.reshape(1), jnp.stack(owners), home, *weights)

    place = jnp.stack([lane, core])
    first = pl.BlockSpec((1024, 256), lambda i: (0, 0))
    early = kernel(
        early_kernel,
        shape((2048, 256), F32),
        670 << 20,
        grid=(1,),
        in_specs=[scalars, first] + [whole] * len(EARLY),
        out_specs=whole,
    )(place, in_hbm(grads), own, deep, own_before, own_after, own_last)

    def late(side, out_shape):
        return kernel(
            functools.partial(late_kernel, side),
            out_shape,
            200 << 20,
            grid=(1,),
            in_specs=[scalars, first] + [whole] * (1 + len(LATE)),
            out_specs=whole,
        )(place, in_hbm(grads), early, deep_last, deep_before, deep_after)

    piece = (2048 // ring // cores, 256)
    sends = []
    if cores == 2:
        theirs = late(1, pltpu.HBM((ring, *piece), BF16))
        theirs = lax.ppermute(theirs, "dp_1", [(0, 1), (1, 0)])
    terms = late(0, shape((ring, *piece), F32))
    if cores == 2:
        terms, *sends = kernel(
            core_sum_kernel,
            [shape(piece, F32)] + [shape(piece, BF16)] * (ring - 1),
            1 << 20,
            in_specs=[scalars] + [whole] * 2,
            out_specs=[whole] * ring,
        )(turn.reshape(1), terms, theirs)
        for step in range(1, ring):
            moves = [(i, (i + step) % ring) for i in range(ring)]
            sends[step - 1] = lax.ppermute(sends[step - 1], "dp_0", moves)
    mine, theirs = kernel(ring_sum_kernel, (shape(piece, F32), shape(piece, BF16)), 1 << 20)(
        terms.reshape(piece), *sends
    )
    theirs = lax.ppermute(theirs, SP, [(u, u ^ 12) for u in range(peers)])
    spread = kernel(half_sum_kernel, pltpu.HBM((8, *piece), BF16), 1 << 20)(mine, theirs)
    spread = lax.all_to_all(spread, "lane", 0, 0, tiled=True)
    grad_weight = kernel(
        widen_kernel,
        pltpu.HBM((piece[0], 2048), F32),
        1 << 20,
        in_specs=[scalars, whole],
        out_specs=whole,
    )(half.reshape(1), spread)
    return grad_query[None], grad_value[None], grad_input[None], grad_weight


def solution(mesh):
    dp = mesh.shape["dp"]
    outer = (dp // 2, 2) if dp > 1 else (1, 1)
    finer = Mesh(mesh.devices.reshape(2, 8, *outer), SP + DP)
    part = P(DP, SP, None)
    return jax.shard_map(
        shards,
        mesh=finer,
        in_specs=(part, part, part, part, part, part, P(DP, None)),
        out_specs=(part, part, part, P(DP, None)),
        check_vma=False,
    )
```

```python
import functools

import jax
import jax.numpy as jnp
from jax import lax
from jax.experimental import pallas as pl
from jax.experimental.pallas import tpu as pltpu
from jax.sharding import Mesh
from jax.sharding import PartitionSpec as P


HEADS = 8
BLOCK = 128
TILE = 256
SP = ("half", "lane")
DP = ("dp_0", "dp_1")
F32 = jnp.float32
BF16 = jnp.bfloat16


def dot(a, b, dims, precision=None):
    return lax.dot_general(a, b, (dims, ((), ())), precision=precision, preferred_element_type=F32)


NN = ((1,), (0,))
NT = ((1,), (1,))
TN = ((0,), (0,))


def decay_kernel(lam_ref, half_ref, rows_ref, factors_ref):
    n = BLOCK
    row = lax.broadcasted_iota(jnp.int32, (n, n), 0)
    col = lax.broadcasted_iota(jnp.int32, (n, n), 1)
    lam = lam_ref[...]
    high = lax.Precision.HIGHEST
    upto = dot(lam, (row <= col).astype(F32), NN, high)
    before = dot(lam, (row < col).astype(F32), NN, high)
    since = dot(lam, (row >= col).astype(F32), NN, high)
    after = dot(lam, (row > col).astype(F32), NN, high)
    totals = [jnp.broadcast_to(upto[b : b + 1, n - 1 : n], (1, n)) for b in range(16)]
    loc0, suf1, rem0, pre1 = [], [], [], []
    for b in range(8):
        odd = b % 2 == 1
        loc0.append(upto[b : b + 1] + totals[b - 1] if odd else upto[b : b + 1])
        suf1.append(since[8 + b : 9 + b] if odd else since[8 + b : 9 + b] + totals[9 + b])
        rem0.append(after[b : b + 1] if odd else after[b : b + 1] + totals[b + 1])
        pre1.append(before[8 + b : 9 + b] + totals[7 + b] if odd else before[8 + b : 9 + b])
    tile0 = [totals[2 * t] + totals[2 * t + 1] for t in range(4)]
    tile1 = [totals[8 + 2 * t] + totals[9 + 2 * t] for t in range(4)]
    first = half_ref[...] == 0
    key_sum, query_sum = [], []
    for b in range(8):
        t = b // 2
        later0, later1 = sum(tile0[t + 1 :]), sum(tile1[t + 1 :])
        early0, early1 = sum(tile0[:t]), sum(tile1[:t])
        key_sum.append(jnp.where(first, rem0[b] + later0, pre1[b] + early1))
        query_sum.append(jnp.where(first, suf1[b] + later1, loc0[b] + early0))
    rows_ref[...] = jnp.concatenate(loc0 + suf1 + rem0 + pre1 + tile0 + tile1, axis=0)
    tiles = []
    for t in range(4):
        pair = slice(2 * t, 2 * t + 2)
        tiles += [jnp.exp(k) for k in key_sum[pair]]
        tiles += [jnp.exp(q) * 0.0625 for q in query_sum[pair]]
        tiles += loc0[pair] + suf1[pair]
    factors_ref[...] = jnp.concatenate(tiles, axis=0)


def upright(factors):
    turned = jnp.transpose(factors)
    pairs = [(turned[:, 2 * k : 2 * k + 1], turned[:, 2 * k + 1 : 2 * k + 2]) for k in range(4)]
    return [jnp.concatenate(pair, axis=0) for pair in pairs]


def wide(rows, base, t):
    return jnp.concatenate([rows[base + 2 * t : base + 2 * t + 1], rows[base + 2 * t + 1 : base + 2 * t + 2]], axis=1)


def boundary_kernel(units_ref, factors_ref, state_ref):
    sides = [upright(factors_ref[8 * t : 8 * t + 8, :]) for t in range(4)]
    to_end = jnp.concatenate([side[0] for side in sides], axis=0)
    from_end = jnp.concatenate([side[1] for side in sides], axis=0)
    keys = (units_ref[:, 256:512].astype(F32) * to_end).astype(BF16)
    queries = (units_ref[:, 0:256].astype(F32) * from_end).astype(BF16)
    state_ref[0] = dot(keys, units_ref[:, 512:1024], TN).astype(BF16)
    state_ref[1] = dot(queries, units_ref[:, 1024:1536], TN).astype(BF16)


def inside_kernel(units_ref, rows_ref, factors_ref, out_ref, s_ref, gs_ref):
    rows = rows_ref[...]
    row = lax.broadcasted_iota(jnp.int32, (TILE, TILE), 0)
    col = lax.broadcasted_iota(jnp.int32, (TILE, TILE), 1)
    for i in range(4):
        at = pl.ds(i * TILE, TILE)
        query, grad = units_ref[at, 0:256], units_ref[at, 1024:1536]
        loc0, suf1 = upright(factors_ref[8 * i : 8 * i + 8, :])[2:]
        for j in range(4):
            to = pl.ds(j * TILE, TILE)
            if i == j:
                spread = jnp.where(row >= col, loc0 - wide(rows, 0, i), suf1 - wide(rows, 8, i))
            elif i > j:
                along = wide(rows, 16, j)
                for t in range(j + 1, i):
                    along = along + jnp.concatenate([rows[32 + t : 33 + t]] * 2, axis=1)
                spread = loc0 + along
            else:
                along = wide(rows, 24, j)
                for t in range(i + 1, j):
                    along = along + jnp.concatenate([rows[36 + t : 37 + t]] * 2, axis=1)
                spread = suf1 + along
            weights = jnp.exp(spread) * 0.0625
            scores = dot(query, units_ref[to, 256:512], NT)
            grads = dot(grad, units_ref[to, 512:1024], NT)
            s_ref[at, to] = (scores * weights).astype(BF16)
            gs_ref[at, to] = (grads * weights).astype(BF16)
    out_ref[:, 0:256] = dot(gs_ref[...], units_ref[:, 0:256], TN).astype(BF16)
    out_ref[:, 256:512] = dot(gs_ref[...], units_ref[:, 256:512], NN).astype(BF16)
    out_ref[:, 512:1024] = dot(s_ref[...], units_ref[:, 1024:1536], TN).astype(BF16)


def across_kernel(units_ref, factors_ref, state_ref, part_ref, out_ref):
    memory, later = state_ref[0], state_ref[1]
    to_end, from_end = upright(factors_ref[...])[:2]
    keys = (units_ref[:, 256:512].astype(F32) * to_end).astype(BF16)
    part = dot(units_ref[:, 512:1024], later, NT) * to_end
    out_ref[:, 0:256] = (part_ref[:, 0:256].astype(F32) + part).astype(BF16)
    part = dot(units_ref[:, 1024:1536], memory, NT) * from_end
    out_ref[:, 256:512] = (part_ref[:, 256:512].astype(F32) + part).astype(BF16)
    part = dot(keys, later, NN)
    out_ref[:, 512:1024] = (part_ref[:, 512:1024].astype(F32) + part).astype(BF16)


def kernel(body, out_shape, flops, scratch=(), **grid):
    return pl.pallas_call(
        body,
        out_shape=out_shape,
        scratch_shapes=scratch,
        cost_estimate=pl.CostEstimate(flops=flops, bytes_accessed=4 << 20, transcendentals=0),
        compiler_params=pltpu.CompilerParams(vmem_limit_bytes=24 << 20),
        **grid,
    )


def in_hbm(array):
    return pltpu.with_memory_space_constraint(array, pltpu.HBM)


def shape(dims, dtype):
    return jax.ShapeDtypeStruct(dims, dtype)


PARTS = 4


def pack_kernel(half_ref, *refs):
    sources, (out_ref,), stages, packed_ref, in_sems, out_sems = (
        refs[:4],
        refs[4:5],
        refs[5:9],
        refs[9],
        refs[10],
        refs[11],
    )
    span = BLOCK // PARTS
    loads, stores = [], []
    for p in range(PARTS):
        rows = pl.ds(p * span, span)
        for k, (source, stage) in enumerate(zip(sources, stages, strict=True)):
            loads.append(
                pltpu.make_async_copy(source.at[rows, :], stage.at[rows, :], in_sems.at[p * 4 + k])
            )
        stores.append(
            pltpu.make_async_copy(packed_ref.at[p], out_ref.at[:, rows, :], out_sems.at[p])
        )
    for load in loads:
        load.start()
    for p in range(PARTS):
        rows = pl.ds(p * span, span)
        for load in loads[4 * p : 4 * p + 4]:
            load.wait()
        for h in range(HEADS):
            lane, at = (h + 4 * half_ref[0]) & 7, 0
            for stage in stages:
                width = stage.shape[1] // HEADS
                packed_ref[p, lane, :, at : at + width] = stage[rows, h * width : h * width + width]
                at += width
        stores[p].start()
    for store in stores:
        store.wait()


def pack(half, arrays):
    outside = pl.BlockSpec(memory_space=pltpu.HBM)
    return pl.pallas_call(
        pack_kernel,
        out_shape=pltpu.HBM((HEADS, BLOCK, 1536), BF16),
        in_specs=[pl.BlockSpec(memory_space=pltpu.SMEM)] + [outside] * 4,
        out_specs=outside,
        scratch_shapes=[
            *[pltpu.VMEM(a.shape, BF16) for a in arrays],
            pltpu.VMEM((PARTS, HEADS, BLOCK // PARTS, 1536), BF16),
            pltpu.SemaphoreType.DMA((4 * PARTS,)),
            pltpu.SemaphoreType.DMA((PARTS,)),
        ],
        cost_estimate=pl.CostEstimate(flops=1 << 20, bytes_accessed=6 << 20, transcendentals=0),
        compiler_params=pltpu.CompilerParams(vmem_limit_bytes=16 << 20),
    )(half.reshape(1), *[in_hbm(a) for a in arrays])


def worker(half, head):
    return half * 8 + (head + 4 * half) % 8


EARLY = ((0, 0), (1, 0), (0, 3), (0, 1), (0, 2), (1, 2))
LATE = ((1, 3), (1, 1))


def term_sum(lane, grads_ref, pieces, steps, total):
    deep, y = lane // 4, lane % 4
    for piece, (other, step) in zip(pieces, steps, strict=True):
        block = (deep ^ other) * 4 + (y + step) % 4
        grad = grads_ref[pl.ds(pl.multiple_of(block * BLOCK, BLOCK), BLOCK), :]
        part = dot(piece[0], grad, TN)
        total = part if total is None else total + part
    return total


def early_kernel(place_ref, grads_ref, *refs):
    refs[-1][...] = term_sum(place_ref[0], grads_ref, refs[:-1], EARLY, None)


def late_kernel(side, place_ref, grads_ref, early_ref, *refs):
    pieces, out_ref = refs[:-1], refs[-1]
    ring, span, _ = out_ref.shape
    cores = early_ref.shape[0] // (ring * span)
    lane = place_ref[0]
    deep, y = lane // 4, lane % 4
    grads = []
    for other, step in LATE:
        block = (deep ^ other) * 4 + (y + step) % 4
        grads.append(grads_ref[pl.ds(pl.multiple_of(block * BLOCK, BLOCK), BLOCK), :])
    for k in range(ring):
        owner = cores * k + (place_ref[1] if side == 0 else 1 - place_ref[1])
        at = pl.multiple_of(owner * span, span)
        total = early_ref[pl.ds(at, span), :]
        for piece, grad in zip(pieces, grads, strict=True):
            total = total + dot(piece[0, :, pl.ds(at, span)], grad, TN)
        out_ref[k] = total.astype(out_ref.dtype)


def core_sum_kernel(turn_ref, mine_ref, theirs_ref, own_ref, *send_refs):
    ring = mine_ref.shape[0]
    for step, ref in enumerate((own_ref, *send_refs)):
        at = (turn_ref[0] + step) & (ring - 1)
        ref[...] = (mine_ref[at] + theirs_ref[at].astype(F32)).astype(ref.dtype)


def ring_sum_kernel(*refs):
    total = refs[0][...]
    for ref in refs[1:-2]:
        total = total + ref[...].astype(F32)
    refs[-2][...] = total
    refs[-1][...] = total.astype(BF16)


def half_sum_kernel(mine_ref, theirs_ref, out_ref):
    total = (mine_ref[...] + theirs_ref[...].astype(F32)).astype(BF16)
    for k in range(out_ref.shape[0]):
        out_ref[k] = total


def home_kernel(half_ref, owner_ref, home_ref, *refs):
    weights, (query_ref, value_ref, input_ref, key_ref) = refs[:-4], refs[-4:]
    for h in range(HEADS):
        lane = (h + 4 * half_ref[0]) & 7
        key_ref[:, h * 256 : h * 256 + 256] = home_ref[lane, :, 0:256]
        query_ref[:, h * 256 : h * 256 + 256] = home_ref[lane, :, 256:512]
        value_ref[:, h * 512 : h * 512 + 512] = home_ref[lane, :, 512:1024]
    for k, weight in enumerate(weights):
        span = weight.shape[0]
        at = pl.multiple_of(owner_ref[k] * span, span)
        input_ref[:, pl.ds(at, span)] = dot(key_ref[...], weight[...], NT).astype(BF16)


def widen_kernel(half_ref, in_ref, out_ref):
    for k in range(HEADS):
        at = pl.multiple_of(((k + 4 * half_ref[0]) & 7) * 256, 256)
        out_ref[:, pl.ds(at, 256)] = in_ref[k].astype(F32)


def shards(layer_input, queries, key_vectors, values, cotangent, log_decay, key_weight):
    tokens = layer_input.shape[1]
    half = lax.axis_index("half")
    lane = lax.axis_index("lane")
    peers = lax.axis_size(SP)
    ring = lax.axis_size("dp_0")
    cores = lax.axis_size("dp_1")
    core, turn = lax.axis_index("dp_1"), lax.axis_index("dp_0")

    decay = log_decay.reshape(2, 8, BLOCK)
    own = lane % 2
    near = lax.dynamic_index_in_dim(decay, own, 0, keepdims=False)
    far = lax.dynamic_index_in_dim(decay, 1 - own, 0, keepdims=False)
    near = lax.ppermute(near, SP, [(u, worker(u % 2, u // 2)) for u in range(peers)])
    far = lax.ppermute(far, SP, [(u, worker(1 - u % 2, u // 2)) for u in range(peers)])
    deep = lax.ppermute(layer_input, "lane", [(i, (i + 4) % 8) for i in range(8)])
    lam = jnp.where(half == 0, jnp.concatenate([near, far]), jnp.concatenate([far, near]))
    rows, factors = kernel(decay_kernel, (shape((40, 128), F32), shape((32, 128), F32)), 1 << 20)(
        lam, jnp.full((1, 128), half, jnp.int32)
    )

    whole = pl.BlockSpec(memory_space=pltpu.VMEM)
    scalars = pl.BlockSpec(memory_space=pltpu.SMEM)
    sent = pack(half, [a[0] for a in (queries, key_vectors, values, cotangent)])
    units = lax.all_to_all(sent, "lane", 0, 0, tiled=True).reshape(8 * tokens, -1)

    def lane_step(array, step):
        return lax.ppermute(
            array, "lane", [(i, i // 4 * 4 + (i + step) % 4) for i in range(8)]
        )

    weights, owners = [key_weight], [turn * cores + core]
    for step in range(1, ring):
        moves = [(i, (i + step) % ring) for i in range(ring)]
        weights.append(lax.ppermute(key_weight, "dp_0", moves))
        owners.append((turn - step) % ring * cores + core)
    if cores == 2:
        weights += [lax.ppermute(w, "dp_1", [(0, 1), (1, 0)]) for w in weights]
        owners += [o + 1 - 2 * core for o in owners]

    own = layer_input
    own_last = lane_step(own, 2)
    own_before, own_after = lane_step(own, 1), lane_step(own, 3)
    deep_before, deep_after = lane_step(deep, 1), lane_step(deep, 3)
    deep_last = lax.ppermute(own_last, "lane", [(i, (i + 4) % 8) for i in range(8)])

    state = kernel(boundary_kernel, pltpu.HBM((2, 256, 512), BF16), 540 << 20)(units, factors)
    state = lax.ppermute(state, SP, [(u, u ^ 12) for u in range(peers)])
    part = kernel(
        inside_kernel,
        pltpu.HBM((1024, 1024), BF16),
        3760 << 20,
        (pltpu.VMEM((1024, 1024), BF16), pltpu.VMEM((1024, 1024), BF16)),
    )(units, rows, factors)

    def by_tile(width):
        return pl.BlockSpec((TILE, width), lambda i: (i, 0))

    grads = kernel(
        across_kernel,
        pltpu.HBM((1024, 1024), BF16),
        800 << 20,
        grid=(4,),
        in_specs=[
            by_tile(1536),
            pl.BlockSpec((8, 128), lambda i: (i, 0)),
            pl.BlockSpec((2, 256, 512), lambda i: (0, 0, 0)),
            by_tile(1024),
        ],
        out_specs=by_tile(1024),
    )(units, factors, state, in_hbm(part))

    home = lax.all_to_all(grads.reshape(8, tokens, -1), "lane", 0, 0, tiled=True)
    grad_query, grad_value, grad_input = kernel(
        home_kernel,
        (shape((tokens, 2048), BF16), shape((tokens, 4096), BF16), shape((tokens, 2048), BF16)),
        1070 << 20,
        (pltpu.VMEM((tokens, 2048), BF16),),
        in_specs=[scalars] * 2 + [whole] * (1 + len(weights)),
        out_specs=(whole, whole, whole),
    )(half.reshape(1), jnp.stack(owners), home, *weights)

    place = jnp.stack([lane, core])
    first = pl.BlockSpec((1024, 256), lambda i: (0, 0))
    early = kernel(
        early_kernel,
        shape((2048, 256), F32),
        670 << 20,
        grid=(1,),
        in_specs=[scalars, first] + [whole] * len(EARLY),
        out_specs=whole,
    )(place, in_hbm(grads), own, deep, own_before, own_after, own_last, deep_last)

    def late(side, out_shape):
        return kernel(
            functools.partial(late_kernel, side),
            out_shape,
            200 << 20,
            grid=(1,),
            in_specs=[scalars, first] + [whole] * (1 + len(LATE)),
            out_specs=whole,
        )(place, in_hbm(grads), early, deep_before, deep_after)

    piece = (2048 // ring // cores, 256)
    sends = []
    if cores == 2:
        theirs = late(1, pltpu.HBM((ring, *piece), BF16))
        theirs = lax.ppermute(theirs, "dp_1", [(0, 1), (1, 0)])
    terms = late(0, shape((ring, *piece), F32))
    if cores == 2:
        terms, *sends = kernel(
            core_sum_kernel,
            [shape(piece, F32)] + [shape(piece, BF16)] * (ring - 1),
            1 << 20,
            in_specs=[scalars] + [whole] * 2,
            out_specs=[whole] * ring,
        )(turn.reshape(1), terms, theirs)
        for step in range(1, ring):
            moves = [(i, (i + step) % ring) for i in range(ring)]
            sends[step - 1] = lax.ppermute(sends[step - 1], "dp_0", moves)
    mine, theirs = kernel(ring_sum_kernel, (shape(piece, F32), shape(piece, BF16)), 1 << 20)(
        terms.reshape(piece), *sends
    )
    theirs = lax.ppermute(theirs, SP, [(u, u ^ 12) for u in range(peers)])
    spread = kernel(half_sum_kernel, pltpu.HBM((8, *piece), BF16), 1 << 20)(mine, theirs)
    spread = lax.all_to_all(spread, "lane", 0, 0, tiled=True)
    grad_weight = kernel(
        widen_kernel,
        pltpu.HBM((piece[0], 2048), F32),
        1 << 20,
        in_specs=[scalars, whole],
        out_specs=whole,
    )(half.reshape(1), spread)
    return grad_query[None], grad_value[None], grad_input[None], grad_weight


def solution(mesh):
    dp = mesh.shape["dp"]
    outer = (dp // 2, 2) if dp > 1 else (1, 1)
    finer = Mesh(mesh.devices.reshape(2, 8, *outer), SP + DP)
    part = P(DP, SP, None)
    return jax.shard_map(
        shards,
        mesh=finer,
        in_specs=(part, part, part, part, part, part, P(DP, None)),
        out_specs=(part, part, part, P(DP, None)),
        check_vma=False,
    )
```

```python
import functools

import jax
import jax.numpy as jnp
from jax import lax
from jax.experimental import pallas as pl
from jax.experimental.pallas import tpu as pltpu
from jax.sharding import Mesh
from jax.sharding import PartitionSpec as P


HEADS = 8
BLOCK = 128
TILE = 256
SP = ("half", "lane")
DP = ("dp_0", "dp_1")
F32 = jnp.float32
BF16 = jnp.bfloat16


def dot(a, b, dims, precision=None):
    return lax.dot_general(a, b, (dims, ((), ())), precision=precision, preferred_element_type=F32)


NN = ((1,), (0,))
NT = ((1,), (1,))
TN = ((0,), (0,))


def decay_kernel(lam_ref, half_ref, rows_ref, factors_ref):
    n = BLOCK
    row = lax.broadcasted_iota(jnp.int32, (n, n), 0)
    col = lax.broadcasted_iota(jnp.int32, (n, n), 1)
    lam = lam_ref[...]
    high = lax.Precision.HIGHEST
    upto = dot(lam, (row <= col).astype(F32), NN, high)
    before = dot(lam, (row < col).astype(F32), NN, high)
    since = dot(lam, (row >= col).astype(F32), NN, high)
    after = dot(lam, (row > col).astype(F32), NN, high)
    totals = [jnp.broadcast_to(upto[b : b + 1, n - 1 : n], (1, n)) for b in range(16)]
    loc0, suf1, rem0, pre1 = [], [], [], []
    for b in range(8):
        odd = b % 2 == 1
        loc0.append(upto[b : b + 1] + totals[b - 1] if odd else upto[b : b + 1])
        suf1.append(since[8 + b : 9 + b] if odd else since[8 + b : 9 + b] + totals[9 + b])
        rem0.append(after[b : b + 1] if odd else after[b : b + 1] + totals[b + 1])
        pre1.append(before[8 + b : 9 + b] + totals[7 + b] if odd else before[8 + b : 9 + b])
    tile0 = [totals[2 * t] + totals[2 * t + 1] for t in range(4)]
    tile1 = [totals[8 + 2 * t] + totals[9 + 2 * t] for t in range(4)]
    first = half_ref[...] == 0
    key_sum, query_sum = [], []
    for b in range(8):
        t = b // 2
        later0, later1 = sum(tile0[t + 1 :]), sum(tile1[t + 1 :])
        early0, early1 = sum(tile0[:t]), sum(tile1[:t])
        key_sum.append(jnp.where(first, rem0[b] + later0, pre1[b] + early1))
        query_sum.append(jnp.where(first, suf1[b] + later1, loc0[b] + early0))
    rows_ref[...] = jnp.concatenate(loc0 + suf1 + rem0 + pre1 + tile0 + tile1, axis=0)
    tiles = []
    for t in range(4):
        pair = slice(2 * t, 2 * t + 2)
        tiles += [jnp.exp(k) for k in key_sum[pair]]
        tiles += [jnp.exp(q) * 0.0625 for q in query_sum[pair]]
        tiles += loc0[pair] + suf1[pair]
    factors_ref[...] = jnp.concatenate(tiles, axis=0)


def upright(factors):
    turned = jnp.transpose(factors)
    pairs = [(turned[:, 2 * k : 2 * k + 1], turned[:, 2 * k + 1 : 2 * k + 2]) for k in range(4)]
    return [jnp.concatenate(pair, axis=0) for pair in pairs]


def wide(rows, base, t):
    return jnp.concatenate([rows[base + 2 * t : base + 2 * t + 1], rows[base + 2 * t + 1 : base + 2 * t + 2]], axis=1)


def boundary_kernel(units_ref, factors_ref, state_ref):
    sides = [upright(factors_ref[8 * t : 8 * t + 8, :]) for t in range(4)]
    to_end = jnp.concatenate([side[0] for side in sides], axis=0)
    from_end = jnp.concatenate([side[1] for side in sides], axis=0)
    keys = (units_ref[:, 256:512].astype(F32) * to_end).astype(BF16)
    queries = (units_ref[:, 0:256].astype(F32) * from_end).astype(BF16)
    state_ref[0] = dot(keys, units_ref[:, 512:1024], TN).astype(BF16)
    state_ref[1] = dot(queries, units_ref[:, 1024:1536], TN).astype(BF16)


def inside_kernel(units_ref, rows_ref, factors_ref, out_ref, s_ref, gs_ref):
    rows = rows_ref[...]
    row = lax.broadcasted_iota(jnp.int32, (TILE, TILE), 0)
    col = lax.broadcasted_iota(jnp.int32, (TILE, TILE), 1)
    for i in range(4):
        at = pl.ds(i * TILE, TILE)
        query, grad = units_ref[at, 0:256], units_ref[at, 1024:1536]
        loc0, suf1 = upright(factors_ref[8 * i : 8 * i + 8, :])[2:]
        for j in range(4):
            to = pl.ds(j * TILE, TILE)
            if i == j:
                spread = jnp.where(row >= col, loc0 - wide(rows, 0, i), suf1 - wide(rows, 8, i))
            elif i > j:
                along = wide(rows, 16, j)
                for t in range(j + 1, i):
                    along = along + jnp.concatenate([rows[32 + t : 33 + t]] * 2, axis=1)
                spread = loc0 + along
            else:
                along = wide(rows, 24, j)
                for t in range(i + 1, j):
                    along = along + jnp.concatenate([rows[36 + t : 37 + t]] * 2, axis=1)
                spread = suf1 + along
            weights = jnp.exp(spread) * 0.0625
            scores = dot(query, units_ref[to, 256:512], NT)
            grads = dot(grad, units_ref[to, 512:1024], NT)
            s_ref[at, to] = (scores * weights).astype(BF16)
            gs_ref[at, to] = (grads * weights).astype(BF16)
    out_ref[:, 0:256] = dot(gs_ref[...], units_ref[:, 0:256], TN).astype(BF16)
    out_ref[:, 256:512] = dot(gs_ref[...], units_ref[:, 256:512], NN).astype(BF16)
    out_ref[:, 512:1024] = dot(s_ref[...], units_ref[:, 1024:1536], TN).astype(BF16)


def across_kernel(units_ref, factors_ref, state_ref, part_ref, out_ref):
    memory, later = state_ref[0], state_ref[1]
    to_end, from_end = upright(factors_ref[...])[:2]
    keys = (units_ref[:, 256:512].astype(F32) * to_end).astype(BF16)
    part = dot(units_ref[:, 512:1024], later, NT) * to_end
    out_ref[:, 0:256] = (part_ref[:, 0:256].astype(F32) + part).astype(BF16)
    part = dot(units_ref[:, 1024:1536], memory, NT) * from_end
    out_ref[:, 256:512] = (part_ref[:, 256:512].astype(F32) + part).astype(BF16)
    part = dot(keys, later, NN)
    out_ref[:, 512:1024] = (part_ref[:, 512:1024].astype(F32) + part).astype(BF16)


def kernel(body, out_shape, flops, scratch=(), **grid):
    return pl.pallas_call(
        body,
        out_shape=out_shape,
        scratch_shapes=scratch,
        cost_estimate=pl.CostEstimate(flops=flops, bytes_accessed=4 << 20, transcendentals=0),
        compiler_params=pltpu.CompilerParams(vmem_limit_bytes=24 << 20),
        **grid,
    )


def in_hbm(array):
    return pltpu.with_memory_space_constraint(array, pltpu.HBM)


def shape(dims, dtype):
    return jax.ShapeDtypeStruct(dims, dtype)


PARTS = 4


def pack_kernel(half_ref, *refs):
    sources, (out_ref,), stages, packed_ref, in_sems, out_sems = (
        refs[:4],
        refs[4:5],
        refs[5:9],
        refs[9],
        refs[10],
        refs[11],
    )
    span = BLOCK // PARTS
    loads, stores = [], []
    for p in range(PARTS):
        rows = pl.ds(p * span, span)
        for k, (source, stage) in enumerate(zip(sources, stages, strict=True)):
            loads.append(
                pltpu.make_async_copy(source.at[rows, :], stage.at[rows, :], in_sems.at[p * 4 + k])
            )
        stores.append(
            pltpu.make_async_copy(packed_ref.at[p], out_ref.at[:, rows, :], out_sems.at[p])
        )
    for load in loads:
        load.start()
    for p in range(PARTS):
        rows = pl.ds(p * span, span)
        for load in loads[4 * p : 4 * p + 4]:
            load.wait()
        for h in range(HEADS):
            lane, at = (h + 4 * half_ref[0]) & 7, 0
            for stage in stages:
                width = stage.shape[1] // HEADS
                packed_ref[p, lane, :, at : at + width] = stage[rows, h * width : h * width + width]
                at += width
        stores[p].start()
    for store in stores:
        store.wait()


def pack(half, arrays):
    outside = pl.BlockSpec(memory_space=pltpu.HBM)
    return pl.pallas_call(
        pack_kernel,
        out_shape=pltpu.HBM((HEADS, BLOCK, 1536), BF16),
        in_specs=[pl.BlockSpec(memory_space=pltpu.SMEM)] + [outside] * 4,
        out_specs=outside,
        scratch_shapes=[
            *[pltpu.VMEM(a.shape, BF16) for a in arrays],
            pltpu.VMEM((PARTS, HEADS, BLOCK // PARTS, 1536), BF16),
            pltpu.SemaphoreType.DMA((4 * PARTS,)),
            pltpu.SemaphoreType.DMA((PARTS,)),
        ],
        cost_estimate=pl.CostEstimate(flops=1 << 20, bytes_accessed=6 << 20, transcendentals=0),
        compiler_params=pltpu.CompilerParams(vmem_limit_bytes=16 << 20),
    )(half.reshape(1), *[in_hbm(a) for a in arrays])


def worker(half, head):
    return half * 8 + (head + 4 * half) % 8


EARLY = ((0, 0), (1, 0), (0, 3), (0, 1), (0, 2), (1, 2))
LATE = ((1, 3), (1, 1))


def term_sum(lane, grads_ref, pieces, steps, total):
    deep, y = lane // 4, lane % 4
    for piece, (other, step) in zip(pieces, steps, strict=True):
        block = (deep ^ other) * 4 + (y + step) % 4
        grad = grads_ref[pl.ds(pl.multiple_of(block * BLOCK, BLOCK), BLOCK), :]
        part = dot(piece[0], grad, TN)
        total = part if total is None else total + part
    return total


def early_kernel(place_ref, grads_ref, *refs):
    pieces, out_ref, late_ref = refs[:-2], refs[-2], refs[-1]
    lane = place_ref[0]
    for k, (other, step) in enumerate(LATE):
        block = (lane // 4 ^ other) * 4 + (lane % 4 + step) % 4
        late_ref[k] = grads_ref[pl.ds(pl.multiple_of(block * BLOCK, BLOCK), BLOCK), :]
    out_ref[...] = term_sum(lane, grads_ref, pieces, EARLY, None)


def late_kernel(side, place_ref, grads_ref, early_ref, *refs):
    pieces, out_ref = refs[:-1], refs[-1]
    ring, span, _ = out_ref.shape
    cores = early_ref.shape[0] // (ring * span)
    grads = [grads_ref[k] for k in range(len(LATE))]
    for k in range(ring):
        owner = cores * k + (place_ref[1] if side == 0 else 1 - place_ref[1])
        at = pl.multiple_of(owner * span, span)
        total = early_ref[pl.ds(at, span), :]
        for piece, grad in zip(pieces, grads, strict=True):
            total = total + dot(piece[0, :, pl.ds(at, span)], grad, TN)
        out_ref[k] = total.astype(out_ref.dtype)


def core_sum_kernel(turn_ref, mine_ref, theirs_ref, own_ref, *send_refs):
    ring = mine_ref.shape[0]
    for step, ref in enumerate((own_ref, *send_refs)):
        at = (turn_ref[0] + step) & (ring - 1)
        ref[...] = (mine_ref[at] + theirs_ref[at].astype(F32)).astype(ref.dtype)


def ring_sum_kernel(*refs):
    total = refs[0][...]
    for ref in refs[1:-2]:
        total = total + ref[...].astype(F32)
    refs[-2][...] = total
    refs[-1][...] = total.astype(BF16)


def half_sum_kernel(mine_ref, theirs_ref, out_ref):
    total = (mine_ref[...] + theirs_ref[...].astype(F32)).astype(BF16)
    for k in range(out_ref.shape[0]):
        out_ref[k] = total


def home_kernel(half_ref, owner_ref, home_ref, *refs):
    weights, (query_ref, value_ref, input_ref, key_ref) = refs[:-4], refs[-4:]
    for h in range(HEADS):
        lane = (h + 4 * half_ref[0]) & 7
        key_ref[:, h * 256 : h * 256 + 256] = home_ref[lane, :, 0:256]
        query_ref[:, h * 256 : h * 256 + 256] = home_ref[lane, :, 256:512]
        value_ref[:, h * 512 : h * 512 + 512] = home_ref[lane, :, 512:1024]
    for k, weight in enumerate(weights):
        span = weight.shape[0]
        at = pl.multiple_of(owner_ref[k] * span, span)
        input_ref[:, pl.ds(at, span)] = dot(key_ref[...], weight[...], NT).astype(BF16)


def widen_kernel(half_ref, in_ref, out_ref):
    for k in range(HEADS):
        at = pl.multiple_of(((k + 4 * half_ref[0]) & 7) * 256, 256)
        out_ref[:, pl.ds(at, 256)] = in_ref[k].astype(F32)


def shards(layer_input, queries, key_vectors, values, cotangent, log_decay, key_weight):
    tokens = layer_input.shape[1]
    half = lax.axis_index("half")
    lane = lax.axis_index("lane")
    peers = lax.axis_size(SP)
    ring = lax.axis_size("dp_0")
    cores = lax.axis_size("dp_1")
    core, turn = lax.axis_index("dp_1"), lax.axis_index("dp_0")

    decay = log_decay.reshape(2, 8, BLOCK)
    own = lane % 2
    near = lax.dynamic_index_in_dim(decay, own, 0, keepdims=False)
    far = lax.dynamic_index_in_dim(decay, 1 - own, 0, keepdims=False)
    near = lax.ppermute(near, SP, [(u, worker(u % 2, u // 2)) for u in range(peers)])
    far = lax.ppermute(far, SP, [(u, worker(1 - u % 2, u // 2)) for u in range(peers)])
    deep = lax.ppermute(layer_input, "lane", [(i, (i + 4) % 8) for i in range(8)])
    lam = jnp.where(half == 0, jnp.concatenate([near, far]), jnp.concatenate([far, near]))
    rows, factors = kernel(decay_kernel, (shape((40, 128), F32), shape((32, 128), F32)), 1 << 20)(
        lam, jnp.full((1, 128), half, jnp.int32)
    )

    whole = pl.BlockSpec(memory_space=pltpu.VMEM)
    scalars = pl.BlockSpec(memory_space=pltpu.SMEM)
    sent = pack(half, [a[0] for a in (queries, key_vectors, values, cotangent)])
    units = lax.all_to_all(sent, "lane", 0, 0, tiled=True).reshape(8 * tokens, -1)

    def lane_step(array, step):
        return lax.ppermute(
            array, "lane", [(i, i // 4 * 4 + (i + step) % 4) for i in range(8)]
        )

    weights, owners = [key_weight], [turn * cores + core]
    for step in range(1, ring):
        moves = [(i, (i + step) % ring) for i in range(ring)]
        weights.append(lax.ppermute(key_weight, "dp_0", moves))
        owners.append((turn - step) % ring * cores + core)
    if cores == 2:
        weights += [lax.ppermute(w, "dp_1", [(0, 1), (1, 0)]) for w in weights]
        owners += [o + 1 - 2 * core for o in owners]

    own = layer_input
    own_last = lane_step(own, 2)
    own_before, own_after = lane_step(own, 1), lane_step(own, 3)
    deep_before, deep_after = lane_step(deep, 1), lane_step(deep, 3)
    deep_last = lax.ppermute(own_last, "lane", [(i, (i + 4) % 8) for i in range(8)])

    state = kernel(boundary_kernel, pltpu.HBM((2, 256, 512), BF16), 540 << 20)(units, factors)
    state = lax.ppermute(state, SP, [(u, u ^ 12) for u in range(peers)])
    part = kernel(
        inside_kernel,
        pltpu.HBM((1024, 1024), BF16),
        3760 << 20,
        (pltpu.VMEM((1024, 1024), BF16), pltpu.VMEM((1024, 1024), BF16)),
    )(units, rows, factors)

    def by_tile(width):
        return pl.BlockSpec((TILE, width), lambda i: (i, 0))

    grads = kernel(
        across_kernel,
        pltpu.HBM((1024, 1024), BF16),
        800 << 20,
        grid=(4,),
        in_specs=[
            by_tile(1536),
            pl.BlockSpec((8, 128), lambda i: (i, 0)),
            pl.BlockSpec((2, 256, 512), lambda i: (0, 0, 0)),
            by_tile(1024),
        ],
        out_specs=by_tile(1024),
    )(units, factors, state, in_hbm(part))

    home = lax.all_to_all(grads.reshape(8, tokens, -1), "lane", 0, 0, tiled=True)
    grad_query, grad_value, grad_input = kernel(
        home_kernel,
        (shape((tokens, 2048), BF16), shape((tokens, 4096), BF16), shape((tokens, 2048), BF16)),
        1070 << 20,
        (pltpu.VMEM((tokens, 2048), BF16),),
        in_specs=[scalars] * 2 + [whole] * (1 + len(weights)),
        out_specs=(whole, whole, whole),
    )(half.reshape(1), jnp.stack(owners), home, *weights)

    place = jnp.stack([lane, core])
    first = pl.BlockSpec((1024, 256), lambda i: (0, 0))
    early, late_grads = kernel(
        early_kernel,
        (shape((2048, 256), F32), shape((len(LATE), BLOCK, 256), BF16)),
        670 << 20,
        grid=(1,),
        in_specs=[scalars, first] + [whole] * len(EARLY),
        out_specs=(whole, whole),
    )(place, in_hbm(grads), own, deep, own_before, own_after, own_last, deep_last)

    def late(side, out_shape):
        return kernel(
            functools.partial(late_kernel, side),
            out_shape,
            200 << 20,
            grid=(1,),
            in_specs=[scalars] + [whole] * (2 + len(LATE)),
            out_specs=whole,
        )(place, late_grads, early, deep_before, deep_after)

    piece = (2048 // ring // cores, 256)
    sends = []
    if cores == 2:
        theirs = late(1, pltpu.HBM((ring, *piece), BF16))
        theirs = lax.ppermute(theirs, "dp_1", [(0, 1), (1, 0)])
    terms = late(0, shape((ring, *piece), F32))
    if cores == 2:
        terms, *sends = kernel(
            core_sum_kernel,
            [shape(piece, F32)] + [shape(piece, BF16)] * (ring - 1),
            1 << 20,
            in_specs=[scalars] + [whole] * 2,
            out_specs=[whole] * ring,
        )(turn.reshape(1), terms, theirs)
        for step in range(1, ring):
            moves = [(i, (i + step) % ring) for i in range(ring)]
            sends[step - 1] = lax.ppermute(sends[step - 1], "dp_0", moves)
    mine, theirs = kernel(ring_sum_kernel, (shape(piece, F32), shape(piece, BF16)), 1 << 20)(
        terms.reshape(piece), *sends
    )
    theirs = lax.ppermute(theirs, SP, [(u, u ^ 12) for u in range(peers)])
    spread = kernel(half_sum_kernel, pltpu.HBM((8, *piece), BF16), 1 << 20)(mine, theirs)
    spread = lax.all_to_all(spread, "lane", 0, 0, tiled=True)
    grad_weight = kernel(
        widen_kernel,
        pltpu.HBM((piece[0], 2048), F32),
        1 << 20,
        in_specs=[scalars, whole],
        out_specs=whole,
    )(half.reshape(1), spread)
    return grad_query[None], grad_value[None], grad_input[None], grad_weight


def solution(mesh):
    dp = mesh.shape["dp"]
    outer = (dp // 2, 2) if dp > 1 else (1, 1)
    finer = Mesh(mesh.devices.reshape(2, 8, *outer), SP + DP)
    part = P(DP, SP, None)
    return jax.shard_map(
        shards,
        mesh=finer,
        in_specs=(part, part, part, part, part, part, P(DP, None)),
        out_specs=(part, part, part, P(DP, None)),
        check_vma=False,
    )
```
